256 devices in a mesh: sp: 16 (over y, x), tp: 16 (over z, core).
Axes of the slice: x: 4, y: 4, z: 8, core: 2. Of those that a mesh axis runs over, the one named last changes fastest.
Arguments:
- queries: bfloat16 [6144, 2048], P('sp', 'tp'), may hold values from -6 to 6
- cell_key_rows: bfloat16 [6144, 2048], P('sp', 'tp'), may hold values from -6 to 6
- cell_value_rows: bfloat16 [6144, 2048], P('sp', 'tp'), may hold values from -6 to 6
- output_gate_logits: bfloat16 [6144, 2048], P('sp', 'tp'), may hold values from -6 to 6
- input_gate_logs: float32 [16, 6144], P('tp', 'sp'), may hold values from -5 to 250
- forget_gate_logits: float32 [16, 6144], P('tp', 'sp'), may hold values from 1 to 13
- extra_log_forget: float32 [16, 6144], P('tp', 'sp'), may hold values from -0.7 to 0
- head_norm_gain: float32 [2048], P('tp'), may hold values from 0.1 to 1.9
- cell_output_matrix: bfloat16 [2048, 4096], P('tp'), may hold values from -0.125 to 0.125
- residual: bfloat16 [6144, 4096], P('sp'), may hold values from -6 to 6
- expert_norm_gain: float32 [4096], replicated, may hold values from 0.1 to 1.9
- routes: int32 [6144, 2], P('sp'), may hold values from 0 to 15, all different within a row; in each aligned block of 24 rows (0 to 23, 24 to 47, ...) at most 6 rows name the same one
- token_expert_weights: float32 [6144, 2], P('sp'), may hold values from 0.2 to 1
- expert_gate_matrix: bfloat16 [16, 4096, 2048], P('sp', None, 'tp'), may hold values from -0.09375 to 0.09375
- expert_up_matrix: bfloat16 [16, 4096, 2048], P('sp', None, 'tp'), may hold values from -0.09375 to 0.09375
- expert_down_matrix: bfloat16 [16, 2048, 4096], P('sp', 'tp'), may hold values from -0.125 to 0.125
Outputs:
- layer_out: bfloat16 [6144, 4096], P(('sp', 'tp'))
The draws below stay inside these ranges and needn't reach their ends.
Inputs may be any that keep to these rules, and one draw needn't show every extreme that they name: `routes`: each row names 2 different experts. In the rows of one device (aligned blocks of 24 rows) no expert is named more than 6 times, and in some blocks one expert is named exactly 6 times.
All inputs are finite; a program needn't handle non-finite values.
Results may differ from the reference program's by a relative error of at most 0.019.
Values may be sent and summed in bfloat16 or wider, within the bound.
A program may use at most 128 MiB of HBM per device.

```python
import math
import jax
import jax.numpy as jnp
import numpy as np
from jax import lax

D = 4096
HEADS = 16
HEAD_DIM = 128
MIX = 2048
FF = 2048
EXPERTS = 16
TOPK = 2
S_DEV = 384
SEQ = 6144
TOK_DEV = 24
CAP = 6
BLOCK = 128
N_TP = 16


def draw_forget_gate_logits(key, part):
    slow_key, shift_key, noise_key = jax.random.split(jax.random.fold_in(key, 11), 3)
    pick = jax.random.uniform(slow_key, (HEADS, 1))
    slow = pick < 0.5
    noise = 0.5 * jnp.clip(jax.random.normal(noise_key, (HEADS, SEQ)), -3.0, 3.0)
    base = jnp.where(slow, jnp.log(2.0 * SEQ), jnp.log(40.0))
    shifts = jax.random.uniform(shift_key, (HEADS, SEQ // S_DEV), minval=-1.0, maxval=1.0)
    return (base + jnp.repeat(shifts, S_DEV, axis=1) + noise).astype(jnp.float32)


def draw_input_gate_logs(key, part):
    base_key = jax.random.fold_in(jax.random.fold_in(key, 13), 0)
    values = jnp.clip(jax.random.normal(base_key, (HEADS, SEQ)), -5.0, 5.0)
    return values.astype(jnp.float32)


def draw_extra_log_forget(key, part):
    place_key, size_key = jax.random.split(jax.random.fold_in(key, 17), 2)
    planted = jax.random.uniform(place_key, (HEADS, SEQ)) < 3.0 / SEQ
    sizes = jnp.log(jax.random.uniform(size_key, (HEADS, SEQ), minval=0.5, maxval=0.8))
    return jnp.where(planted, sizes, 0.0).astype(jnp.float32)


def block_levels(stream_key, shape, shards, least, top_value):
    loudness = 1.0
    for position, shards_of in shards:
        steps = jax.random.uniform(jax.random.fold_in(jax.random.fold_in(stream_key, 6), position), (shards_of,), jnp.float32, least / len(shards), top_value / len(shards))
        loudness = loudness * jnp.repeat(jnp.exp(steps), shape[position] // shards_of).reshape((-1,) + (1,) * (len(shape) - 1 - position))
    return loudness


def assign_block(rng, own, number, rows, amount, top, most, lean):
    order = jax.random.permutation(rng, amount)
    heavy_load, usual = load_shares(amount, rows * top, most, lean, True), load_shares(amount, rows * top, most, lean, False)
    places = jnp.arange(amount)

    def named(tallies, rotation):
        used = int((tallies > 0).sum())
        fixed = max(1, used // 4)
        passed = fixed + (places - fixed + rotation * (used - fixed)) % max(1, amount - fixed)
        return jnp.zeros((amount,), jnp.int32).at[order[jnp.where(places < fixed, places, passed)]].set(jnp.asarray(tallies, jnp.int32))

    tallies = jnp.where(number % 4 == 0, named(heavy_load, number // 4), named(usual, number - number // 4 - 1))
    mixed = jax.random.permutation(jax.random.fold_in(own, 3), amount)
    giver, sink = mixed[0:amount // 2 * 2:2], mixed[1:amount // 2 * 2:2]
    slack = jnp.minimum(tallies[giver] - 1, most - tallies[sink]) // 2
    slack = jnp.where((giver == order[0]) | (sink == order[0]) | (tallies[sink] == 0), 0, jnp.maximum(slack, 0))
    passed = jax.random.randint(jax.random.fold_in(own, 4), (amount // 2,), 0, 1 << 20) % (slack + 1)
    tallies = tallies.at[giver].add(-passed).at[sink].add(passed)
    items = jnp.searchsorted(jnp.cumsum(tallies), jnp.arange(rows * top), side="right").astype(jnp.int32)
    listing = items.reshape(top, rows).T
    listing = listing[jax.random.permutation(jax.random.fold_in(own, 1), rows)]
    rotation = jax.random.randint(jax.random.fold_in(own, 2), (rows, 1), 0, top)
    return jnp.take_along_axis(listing, (jnp.arange(top)[None, :] + rotation) % top, axis=1)


def load_shares(number_of, total, most, slope, full):
    weights = [(1 << 20) // math.isqrt(rank ** slope) + 1 for rank in range(1, number_of + 1)]
    largest = most if full else min(most, max(-(-total // number_of), total * weights[0] // sum(weights)))
    least = 1 if total - largest >= number_of - 1 else 0
    given, rest = [largest] + [least] * (number_of - 1), total - largest - least * (number_of - 1)
    while rest > 0:
        movable = [i for i in range(1, number_of) if given[i] < largest] or [i for i in range(1, number_of) if given[i] < most]
        mass, left = sum([weights[i] for i in movable]), rest
        for i in movable:
            more = min(most - given[i], max(1, left * weights[i] // mass), rest)
            given[i] = given[i] + more
            rest = rest - more
    return np.array(given)


def centred(stream_key, extent, scale, reach, shards=(), held_as=jnp.bfloat16):
    loudness = block_levels(stream_key, extent, shards, -0.22, 0.18) if shards else 1.0
    drawn = jax.random.normal(stream_key, extent, jnp.float32) * scale * loudness
    return jnp.minimum(jnp.maximum(drawn, -reach), reach).astype(held_as)


def setup_inputs(seed: int = 0) -> dict:
    key_list = jax.random.split(jax.random.key(seed), 17)
    queries = centred(key_list[0], (SEQ, MIX), 1.0, 6.0, ((0, 16), (1, 16)))
    cell_key_rows = centred(key_list[1], (SEQ, MIX), 1.0, 6.0, ((0, 16), (1, 16)))
    cell_value_rows = centred(key_list[2], (SEQ, MIX), 1.0, 6.0, ((0, 16), (1, 16)))
    output_gate_logits = centred(key_list[3], (SEQ, MIX), 1.0, 6.0, ((0, 16), (1, 16)))
    input_gate_logs = draw_input_gate_logs(jax.random.fold_in(key_list[16], 71), 0)
    forget_gate_logits = draw_forget_gate_logits(jax.random.fold_in(key_list[16], 71), 0)
    extra_log_forget = draw_extra_log_forget(jax.random.fold_in(key_list[16], 71), 0)
    head_norm_gain = jnp.clip(1.0 + 0.18 * jax.random.normal(key_list[7], (MIX,), jnp.float32), 0.1, 1.9)
    cell_output_matrix = centred(key_list[8], (MIX, D), MIX ** -0.5, 0.125, ((0, 16),))
    residual = centred(key_list[9], (SEQ, D), 1.0, 6.0, ((0, 16),))
    expert_norm_gain = jnp.clip(1.0 + 0.18 * jax.random.normal(key_list[10], (D,), jnp.float32), 0.1, 1.9)
    routes_keys = jax.random.split(jax.random.fold_in(key_list[11], 1), SEQ // TOK_DEV)
    routes_turns = jax.random.permutation(jax.random.fold_in(key_list[11], 3), SEQ // TOK_DEV)
    routes = jax.vmap(lambda own, number: assign_block(jax.random.fold_in(key_list[11], 2), own, number, TOK_DEV, EXPERTS, TOPK, CAP, 2))(routes_keys, routes_turns).reshape((SEQ, TOPK))
    token_expert_weights = jnp.clip(jnp.exp(math.log(1.0) - 1.609438 * jax.random.uniform(key_list[12], (SEQ, TOPK), jnp.float32) ** block_levels(key_list[12], (SEQ, TOPK), ((0, 16),), -0.2, 0.2)), 0.2, 1.0)
    expert_gate_matrix = centred(key_list[13], (EXPERTS, D, FF), D ** -0.5, 0.09375, ((0, 16), (2, 16)))
    expert_up_matrix = centred(key_list[14], (EXPERTS, D, FF), D ** -0.5, 0.09375, ((0, 16), (2, 16)))
    expert_down_matrix = centred(key_list[15], (EXPERTS, FF, D), FF ** -0.5, 0.125, ((0, 16), (1, 16)))
    return dict(queries=queries, cell_key_rows=cell_key_rows, cell_value_rows=cell_value_rows, output_gate_logits=output_gate_logits, input_gate_logs=input_gate_logs, forget_gate_logits=forget_gate_logits, extra_log_forget=extra_log_forget, head_norm_gain=head_norm_gain, cell_output_matrix=cell_output_matrix, residual=residual, expert_norm_gain=expert_norm_gain, routes=routes, token_expert_weights=token_expert_weights, expert_gate_matrix=expert_gate_matrix, expert_up_matrix=expert_up_matrix, expert_down_matrix=expert_down_matrix)


floor_neg = -1e+30
norm_eps = 1e-06
row_group = 128

def block_cells(query_f, key_f, value_f, input_f, forget_log_values, start_cell, start_stab):
    heads, length, width = query_f.shape
    count = length // BLOCK
    highest = lax.Precision.HIGHEST

    def split(array):
        return jnp.moveaxis(array.reshape((heads, count, BLOCK) + array.shape[2:]), 1, 0)
    causal = jnp.tril(jnp.ones((BLOCK, BLOCK), dtype=bool))

    def advance(carry, block):
        cell, stab = carry
        qblock, kblock, vblock, iblock, fblock = block
        cumul = jnp.cumsum(fblock, axis=-1)
        total = cumul[:, -1]
        log_inner = jnp.where(causal[None], cumul[:, :, None] - cumul[:, None, :] + iblock[:, None, :], floor_neg)
        carried = cumul + stab[:, None]
        stab_row = jnp.maximum(carried, lax.optimization_barrier(jnp.max(log_inner, axis=-1)))
        scores = jnp.einsum('hld,hsd->hls', qblock, kblock, precision=highest) * jnp.exp(log_inner - stab_row[..., None])
        numer = jnp.einsum('hls,hsd->hld', scores, vblock, precision=highest) + jnp.exp(carried - stab_row)[..., None] * jnp.einsum('hld,hde->hle', qblock, cell, precision=highest)
        log_write = total[:, None] - cumul + iblock
        stab_next = jnp.maximum(total + stab, lax.optimization_barrier(jnp.max(log_write, axis=-1)))
        weights = jnp.exp(log_write - stab_next[:, None])
        cell_next = jnp.exp(total + stab - stab_next)[:, None, None] * cell + jnp.einsum('hsd,hse->hde', kblock * weights[..., None], vblock, precision=highest)
        return ((cell_next, stab_next), (numer, stab_row))
    inputs = tuple((split(array) for array in (query_f, key_f, value_f, input_f, forget_log_values)))
    unused, (numer, stab_rows) = lax.scan(advance, (start_cell, start_stab), inputs)
    numer = jnp.moveaxis(numer, 0, 1).reshape(heads, length, width)
    stab_rows = jnp.moveaxis(stab_rows, 0, 1).reshape(heads, length)
    return (numer, stab_rows)

def rms_scale(rows, gain):
    values = rows.astype(jnp.float32)
    return (values * lax.rsqrt(lax.optimization_barrier(jnp.mean(values * values, axis=-1, keepdims=True)) + norm_eps) * gain).astype(jnp.bfloat16)

def expert_outputs(moe_in, routes, expert_gate_matrix, expert_up_matrix, expert_down_matrix):
    count = SEQ * TOPK
    expert = routes.reshape(-1).astype(jnp.int32)
    owner = jnp.arange(count, dtype=jnp.int32) // TOPK
    order = jnp.argsort(expert, stable=True).astype(jnp.int32)
    sorted_expert = expert[order]
    loads = lax.optimization_barrier(jnp.sum((expert[:, None] == jnp.arange(EXPERTS, dtype=jnp.int32)[None, :]).astype(jnp.int32), axis=0))
    starts = (jnp.cumsum(loads) - loads).astype(jnp.int32)
    padded = ((loads + row_group - 1) // row_group * row_group).astype(jnp.int32)
    ends = jnp.cumsum(padded).astype(jnp.int32)
    padded_starts = ends - padded
    dest = (padded_starts[sorted_expert] + jnp.arange(count, dtype=jnp.int32) - starts[sorted_expert]).astype(jnp.int32)
    room = (count + row_group - 1) // row_group * row_group + EXPERTS * row_group
    blocks = room // row_group
    row_owner = jnp.full((room,), SEQ, jnp.int32).at[dest].set(owner[order])
    block_first = jnp.arange(blocks, dtype=jnp.int32) * row_group
    block_expert = jnp.minimum(lax.optimization_barrier(jnp.sum((block_first[:, None] >= ends[None, :]).astype(jnp.int32), axis=1)), EXPERTS - 1).astype(jnp.int32)
    padded_in = jnp.concatenate([moe_in, jnp.zeros((1, D), moe_in.dtype)], axis=0)
    block_rows = padded_in[row_owner].reshape(blocks, row_group, D)
    width = FF // N_TP

    def one_block(args):
        rows, which = args
        gate = jnp.dot(rows, expert_gate_matrix[which], preferred_element_type=jnp.float32)
        upper = jnp.dot(rows, expert_up_matrix[which], preferred_element_type=jnp.float32)
        hidden = (jax.nn.silu(gate) * upper).astype(jnp.bfloat16)
        parts = jnp.einsum('rjf,jfd->rjd', hidden.reshape(row_group, N_TP, width).astype(jnp.float32), expert_down_matrix[which].reshape(N_TP, width, D).astype(jnp.float32))
        parts = lax.optimization_barrier(parts.astype(jnp.bfloat16)).astype(jnp.float32)
        return lax.optimization_barrier(jnp.sum(parts, axis=1)).astype(jnp.bfloat16)
    outputs = lax.map(one_block, (block_rows, block_expert)).reshape(room, D)
    place = jnp.zeros((count,), jnp.int32).at[order].set(dest)
    return outputs[place].reshape(SEQ, TOPK, D)

def reference(queries, cell_key_rows, cell_value_rows, output_gate_logits, input_gate_logs, forget_gate_logits, extra_log_forget, head_norm_gain, cell_output_matrix, residual, expert_norm_gain, routes, token_expert_weights, expert_gate_matrix, expert_up_matrix, expert_down_matrix):

    def heads_of(array):
        return jnp.transpose(array.astype(jnp.float32).reshape(SEQ, HEADS, HEAD_DIM), (1, 0, 2))
    query_f = heads_of(queries)
    key_f = heads_of(cell_key_rows) * HEAD_DIM ** (-0.5)
    value_f = heads_of(cell_value_rows)
    forget_log_values = jax.nn.log_sigmoid(forget_gate_logits) + extra_log_forget
    numer, stab_rows = block_cells(query_f, key_f, value_f, input_gate_logs, forget_log_values, jnp.zeros((HEADS, HEAD_DIM, HEAD_DIM), jnp.float32), jnp.zeros((HEADS,), jnp.float32))
    scaled = numer * lax.rsqrt(lax.optimization_barrier(jnp.mean(numer * numer, axis=2, keepdims=True)) + norm_eps) * head_norm_gain.reshape(HEADS, 1, HEAD_DIM)
    mixed = jnp.transpose(scaled, (1, 0, 2)).reshape(SEQ, MIX)
    cell_out = (jax.nn.sigmoid(output_gate_logits.astype(jnp.float32)) * mixed).astype(jnp.bfloat16)
    projected = jnp.dot(cell_out, cell_output_matrix, preferred_element_type=jnp.float32)
    after_mix = (residual.astype(jnp.float32) + projected).astype(jnp.bfloat16)
    moe_in = rms_scale(after_mix, expert_norm_gain)
    chosen = expert_outputs(moe_in, routes, expert_gate_matrix, expert_up_matrix, expert_down_matrix)
    moe = lax.optimization_barrier(jnp.sum(token_expert_weights[:, :, None] * chosen.astype(jnp.float32), axis=1))
    return (after_mix.astype(jnp.float32) + moe).astype(jnp.bfloat16)
```

```python
import jax
import jax.numpy as jnp
from jax import lax
from jax.experimental import pallas as pl
from jax.experimental.pallas import tpu as pltpu
from jax.sharding import PartitionSpec as P

MESH = pl.DeviceIdType.MESH
F32 = jnp.float32
BF16 = jnp.bfloat16

HEAD_DIM = 128
NSP = 16
NZ = 8
LEN = 384
TOK = 24
CAP = 6
GROUPS = 8
WIDE = 512
SLOT = GROUPS * CAP
ROWS = NSP * SLOT
TROWS = GROUPS * TOK
PIECES = 4

floor_neg = -1e30
norm_eps = 1e-06


def dot(a, b):
    return jnp.dot(a, b, preferred_element_type=F32)


def two_parts(x):
    high = x.astype(BF16)
    return high, (x - high.astype(F32)).astype(BF16)


def iota(shape, dim):
    return lax.broadcasted_iota(jnp.int32, shape, dim)


def kernel(
    q_ref, k_ref, v_ref, og_ref, ig_ref, fg_ref, ex_ref, hg_ref,
    resid_ref, eng_ref, tab_ref, rowtab_ref, perm_ref,
    wo_hbm, gate_hbm, up_hbm, down_hbm,
    out_ref,
    wv, gw, dn,
    st_send, st_recv, gs, num_s, co_f, co_a, co_b, co_send, co_recv,
    pf, r1_send, r1_recv, am,
    moe, d_send, d_recv, pin, pout,
    xring, ybuf, t_send, t_recv, r2_send, r2_recv, own,
    load_sem, wx_send, wx_recv, st_ss, st_rs, co_sem, r1_ss, r1_rs,
    d_sem, x_ss, x_rs, t_ss, t_rs, r2_ss, r2_rs,
):
    sp = lax.axis_index("sp")
    tp = lax.axis_index("tp")
    core = lax.rem(tp, 2)
    z = tp // 2
    step = jnp.where(core == 0, 1, NZ - 1)
    after = lax.rem(z + step, NZ) * 2 + core
    before = lax.rem(z + NZ - step, NZ) * 2 + core
    mate = z * 2 + 1 - core

    barrier = pltpu.get_barrier_semaphore()

    @pl.loop(1, NSP)
    def _(i):
        pl.semaphore_signal(
            barrier, inc=1, device_id={"sp": lax.rem(sp + i, NSP), "tp": tp}, device_id_type=MESH
        )

    for other in (after, before, mate):
        pl.semaphore_signal(barrier, inc=1, device_id={"sp": sp, "tp": other}, device_id_type=MESH)

    loads = [
        pltpu.make_async_copy(wo_hbm, wv.at[0], load_sem.at[0]),
        pltpu.make_async_copy(gate_hbm, gw.at[0], load_sem.at[1]),
        pltpu.make_async_copy(up_hbm, gw.at[1], load_sem.at[2]),
        pltpu.make_async_copy(down_hbm, dn.at[0], load_sem.at[3]),
    ]
    for load in loads:
        load.start()

    tt = iota((LEN, LEN), 0)
    ss = iota((LEN, LEN), 1)
    causal = ss <= tt
    fg = fg_ref[...]
    f_row = jnp.minimum(fg, 0.0) - jnp.log1p(jnp.exp(-jnp.abs(fg))) + ex_ref[...]
    i_row = ig_ref[...]
    f_all = jnp.broadcast_to(f_row, (LEN, LEN))
    f_col = jnp.sum(jnp.where(ss == tt, f_all, 0.0), axis=1, keepdims=True)
    i_col = jnp.sum(
        jnp.where(ss == tt, jnp.broadcast_to(i_row, (LEN, LEN)), 0.0), axis=1, keepdims=True
    )
    c_col = jnp.sum(jnp.where(causal, f_all, 0.0), axis=1, keepdims=True)
    c_row = jnp.sum(
        jnp.where(tt <= ss, jnp.broadcast_to(f_col, (LEN, LEN)), 0.0), axis=0, keepdims=True
    )
    total = jnp.sum(f_row, axis=1, keepdims=True)
    scale = HEAD_DIM ** (-0.5)
    write = i_col + total - c_col
    stab_dev = jnp.max(write, axis=0, keepdims=True)
    kw = k_ref[...].astype(F32) * (jnp.exp(write - stab_dev) * scale)
    kw_h, kw_l = two_parts(kw)
    dims = (((0,), (0,)), ((), ()))
    v = v_ref[...]
    st_send[:HEAD_DIM] = lax.dot_general(
        kw_h, v, dims, preferred_element_type=F32
    ) + lax.dot_general(kw_l, v, dims, preferred_element_type=F32)
    st_send[HEAD_DIM:] = jnp.where(
        iota((8, HEAD_DIM), 0) == 0,
        jnp.broadcast_to(stab_dev, (8, HEAD_DIM)),
        jnp.broadcast_to(total, (8, HEAD_DIM)),
    )

    pl.semaphore_wait(barrier, NSP - 1 + 3)

    def state_copy(to, source):
        return pltpu.make_async_remote_copy(
            src_ref=st_send, dst_ref=st_recv.at[source],
            send_sem=st_ss.at[to], recv_sem=st_rs.at[source],
            device_id={"sp": to, "tp": tp}, device_id_type=MESH,
        )

    @pl.loop(sp + 1, NSP)
    def _(to):
        state_copy(to, sp).start()

    pairs = [(wo_hbm, wv.at[1]), (gate_hbm, gw.at[2]), (up_hbm, gw.at[3]), (down_hbm, dn.at[1])]
    shared = [
        pltpu.make_async_remote_copy(
            src_ref=source, dst_ref=target, send_sem=wx_send.at[i], recv_sem=wx_recv.at[i],
            device_id={"sp": sp, "tp": mate}, device_id_type=MESH,
        )
        for i, (source, target) in enumerate(pairs)
    ]
    for copy in shared:
        copy.start()

    q = q_ref[...]
    scores = lax.dot_general(
        q, k_ref[...], (((1,), (1,)), ((), ())), preferred_element_type=F32
    ) * scale
    inner = jnp.where(causal, c_col - c_row + i_row, floor_neg)
    top = jnp.max(inner, axis=1, keepdims=True)
    p_h, p_l = two_parts(scores * jnp.exp(inner - top))
    num_s[...] = dot(p_h, v) + dot(p_l, v)

    col = iota((ROWS, ROWS), 1)
    pin[...] = jnp.where(col == perm_ref[:, 0:1], 1.0, 0.0).astype(BF16)
    pout[...] = jnp.where(col == perm_ref[:, 1:2], 1.0, 0.0).astype(BF16)

    def gather_stab(i, carry):
        stab, tot = carry
        s = sp - 1 - i
        state_copy(s, s).wait_recv()
        here = st_recv[s, HEAD_DIM : HEAD_DIM + 1, :] + tot
        gs[s, 0:1, :] = here
        return jnp.maximum(stab, here), tot + st_recv[s, HEAD_DIM + 1 : HEAD_DIM + 2, :]

    stab0, tot0 = lax.fori_loop(
        0, sp, gather_stab,
        (jnp.full((1, HEAD_DIM), floor_neg, F32), jnp.zeros((1, HEAD_DIM), F32)),
    )
    start_stab = jnp.maximum(stab0, tot0)

    def add_state(s, cell):
        return cell + jnp.exp(gs[s, 0:1, :] - start_stab) * st_recv[s, :HEAD_DIM, :]

    cell_h, cell_l = two_parts(
        lax.fori_loop(0, sp, add_state, jnp.zeros((HEAD_DIM, HEAD_DIM), F32))
    )
    carried = c_col + start_stab[:, 0:1]
    stab = jnp.maximum(top, carried)
    numer = jnp.exp(top - stab) * num_s[...] + jnp.exp(carried - stab) * (
        dot(q, cell_h) + dot(q, cell_l)
    )
    scaled = (
        numer
        * lax.rsqrt(jnp.mean(numer * numer, axis=1, keepdims=True) + norm_eps)
        * hg_ref[...]
    )
    co_f[...] = scaled / (1.0 + jnp.exp(-og_ref[...].astype(F32)))
    for i in range(NZ):
        mine = pl.multiple_of((2 * i + core) * TOK, 8)
        theirs = pl.multiple_of((2 * i + 1 - core) * TOK, 8)
        co_a[i * TOK : (i + 1) * TOK, :] = co_f[pl.ds(mine, TOK), :]
        co_b[i * TOK : (i + 1) * TOK, :] = co_f[pl.ds(theirs, TOK), :]
    co_send[...] = co_b[...].astype(BF16)
    swap = pltpu.make_async_remote_copy(
        src_ref=co_send, dst_ref=co_recv, send_sem=co_sem.at[0], recv_sem=co_sem.at[1],
        device_id={"sp": sp, "tp": mate}, device_id_type=MESH,
    )
    swap.start()
    mine_b = co_a[...].astype(BF16)

    @pl.loop(sp + 1, NSP)
    def _(to):
        state_copy(to, sp).wait_send()

    loads[0].wait()
    shared[0].wait()
    swap.wait()
    theirs_b = co_recv[...]

    @pl.loop(0, GROUPS)
    def _(j):
        at = pl.ds(pl.multiple_of(j * WIDE, WIDE), WIDE)
        part = dot(mine_b, wv[0, :, at]) + dot(theirs_b, wv[1, :, at])
        for i in range(NZ):
            pf[i, pl.ds(pl.multiple_of(j * TOK, 8), TOK), :] = part[i * TOK : (i + 1) * TOK]

    prows = TROWS // PIECES

    def sum_copy(k, p):
        rows = pl.ds(pl.multiple_of(p * prows, prows), prows)
        return pltpu.make_async_remote_copy(
            src_ref=r1_send.at[k, rows], dst_ref=r1_recv.at[k + 1, rows],
            send_sem=r1_ss.at[k, p], recv_sem=r1_rs.at[k + 1, p],
            device_id={"sp": sp, "tp": after}, device_id_type=MESH,
        )

    def block_of(k):
        return lax.rem(z + NZ * NZ - step * k, NZ)

    @pl.loop(1, NZ)
    def _(k):
        block = block_of(k)

        @pl.loop(0, PIECES)
        def _(p):
            rows = pl.ds(pl.multiple_of(p * prows, prows), prows)

            @pl.when(k == 1)
            def _():
                r1_send[k, rows] = pf[block, rows].astype(BF16)

            @pl.when(k > 1)
            def _():
                sum_copy(k - 1, p).wait_recv()
                r1_send[k, rows] = (pf[block, rows] + r1_recv[k, rows].astype(F32)).astype(BF16)

            sum_copy(k, p).start()

    @pl.loop(0, PIECES)
    def _(p):
        sum_copy(NZ - 1, p).wait_recv()

    am[...] = (resid_ref[...].astype(F32) + (pf[z] + r1_recv[NZ].astype(F32))).astype(BF16)

    squares = jnp.zeros((TOK, 1), F32)
    for j in range(GROUPS):
        x = am[...].astype(F32)[j * TOK : (j + 1) * TOK]
        squares = squares + jnp.sum(x * x, axis=1, keepdims=True)
    factor = lax.rsqrt(squares * (1.0 / (GROUPS * WIDE)) + norm_eps)
    moe[...] = jnp.concatenate(
        [
            am[...].astype(F32)[j * TOK : (j + 1) * TOK] * factor * eng_ref[j : j + 1, :]
            for j in range(GROUPS)
        ],
        axis=0,
    ).astype(BF16)
    place = iota((ROWS, TROWS), 0).astype(F32)
    pick = jnp.where(
        (place == rowtab_ref[0:1, :]) | (place == rowtab_ref[1:2, :]), 1.0, 0.0
    ).astype(BF16)
    d_send[...] = dot(pick, moe[...]).astype(BF16)

    def slot_rows(s):
        return pl.ds(pl.multiple_of(s * SLOT, SLOT), SLOT)

    @pl.loop(1, NSP)
    def _(i):
        to = lax.rem(sp + i, NSP)
        pltpu.make_async_remote_copy(
            src_ref=d_send.at[slot_rows(to)], dst_ref=d_recv.at[slot_rows(sp)],
            send_sem=d_sem.at[0], recv_sem=d_sem.at[1],
            device_id={"sp": to, "tp": tp}, device_id_type=MESH,
        ).start()

    d_recv[slot_rows(sp)] = d_send[slot_rows(sp)]

    for load in loads[1:]:
        load.wait()
    for copy in shared[1:]:
        copy.wait()

    others = pl.ds(0, ROWS - SLOT)
    for i in range(2):
        pltpu.make_async_copy(d_recv.at[others], d_recv.at[others], d_sem.at[i]).wait()
    xring[0] = dot(pin[...], d_recv[...]).astype(BF16)

    xrows = ROWS // PIECES
    per = ROWS // GROUPS

    def row_copy(k, p):
        rows = pl.ds(pl.multiple_of(p * xrows, xrows), xrows)
        return pltpu.make_async_remote_copy(
            src_ref=xring.at[k, rows], dst_ref=xring.at[k + 1, rows],
            send_sem=x_ss.at[k, p], recv_sem=x_rs.at[k, p],
            device_id={"sp": sp, "tp": after}, device_id_type=MESH,
        )

    def total_copy(k):
        return pltpu.make_async_remote_copy(
            src_ref=r2_send.at[k], dst_ref=r2_recv.at[k + 1],
            send_sem=r2_ss.at[k], recv_sem=r2_rs.at[k + 1],
            device_id={"sp": sp, "tp": after}, device_id_type=MESH,
        )

    def experts(k):
        acc = jnp.zeros((per, 4 * HEAD_DIM), F32)
        for j in range(GROUPS):
            x = xring[k, j * per : (j + 1) * per, :]
            w = jnp.concatenate([gw[i, j * WIDE : (j + 1) * WIDE, :] for i in range(4)], axis=1)
            acc = acc + dot(x, w)
        acts = []
        for i in range(2):
            gate = acc[:, 2 * i * HEAD_DIM : (2 * i + 1) * HEAD_DIM]
            upper = acc[:, (2 * i + 1) * HEAD_DIM : (2 * i + 2) * HEAD_DIM]
            acts.append((gate / (1.0 + jnp.exp(-gate)) * upper).astype(BF16))
        for j in range(GROUPS):
            at = slice(j * WIDE, (j + 1) * WIDE)
            ybuf[j * per : (j + 1) * per, :] = (
                dot(acts[0], dn[0, :, at]) + dot(acts[1], dn[1, :, at])
            ).astype(BF16)
        t_send[k] = dot(pout[...], ybuf[...]).astype(BF16)

        @pl.loop(1, NSP)
        def _(i):
            to = lax.rem(sp + i, NSP)
            pltpu.make_async_remote_copy(
                src_ref=t_send.at[k, slot_rows(to)], dst_ref=t_recv.at[k, slot_rows(sp)],
                send_sem=t_ss.at[k], recv_sem=t_rs.at[k],
                device_id={"sp": to, "tp": tp}, device_id_type=MESH,
            ).start()

        t_recv[k, slot_rows(sp)] = t_send[k, slot_rows(sp)]

    def combined(k):
        pltpu.make_async_copy(t_recv.at[k, others], t_recv.at[k, others], t_rs.at[k]).wait()
        tab = tab_ref[block_of(k)]
        place = iota((TROWS, ROWS), 1).astype(F32)
        weight = jnp.where(place == tab[:, 0:1], tab[:, 2:3], 0.0) + jnp.where(
            place == tab[:, 1:2], tab[:, 3:4], 0.0
        )
        w_h, w_l = two_parts(weight)
        rows = t_recv[k]
        return dot(w_h, rows) + dot(w_l, rows)

    def combine(k):
        mixed = combined(k)

        @pl.when(k == 0)
        def _():
            own[...] = mixed

        @pl.when(k == 1)
        def _():
            r2_send[k] = mixed.astype(BF16)
            total_copy(k).start()

        @pl.when(k > 1)
        def _():
            total_copy(k - 1).wait_recv()
            r2_send[k] = (mixed + r2_recv[k].astype(F32)).astype(BF16)
            total_copy(k).start()

    @pl.loop(0, NZ)
    def _(k):
        @pl.loop(0, PIECES)
        def _(p):
            @pl.when(k > 0)
            def _():
                row_copy(k - 1, p).wait_recv()

            @pl.when(k < NZ - 1)
            def _():
                row_copy(k, p).start()

        experts(k)

        @pl.when(k > 0)
        def _():
            combine(k - 1)

    combine(NZ - 1)
    total_copy(NZ - 1).wait_recv()
    result = (am[...].astype(F32) + (own[...] + r2_recv[NZ].astype(F32))).astype(BF16).astype(F32)
    for j in range(GROUPS):
        out_ref[:, j * WIDE : (j + 1) * WIDE] = result[j * TOK : (j + 1) * TOK].astype(BF16)

    @pl.loop(1, NZ)
    def _(k):
        total_copy(k).wait_send()

        @pl.loop(0, PIECES)
        def _(p):
            sum_copy(k, p).wait_send()
            row_copy(k - 1, p).wait_send()

    @pl.loop(0, NZ)
    def _(k):
        pltpu.make_async_copy(t_send.at[k, others], t_send.at[k, others], t_ss.at[k]).wait()


def grouped(x):
    rows = x.shape[0]
    return x.reshape(rows, GROUPS, WIDE).transpose(1, 0, 2).reshape(GROUPS * rows, WIDE)


def local(
    queries,
    cell_key_rows,
    cell_value_rows,
    output_gate_logits,
    input_gate_logs,
    forget_gate_logits,
    extra_log_forget,
    head_norm_gain,
    cell_output_matrix,
    residual,
    expert_norm_gain,
    routes,
    token_expert_weights,
    expert_gate_matrix,
    expert_up_matrix,
    expert_down_matrix,
):
    tp = lax.axis_index("tp")
    core, z = tp % 2, tp // 2
    resid = grouped(lax.dynamic_slice_in_dim(residual, tp * TOK, TOK, 0))

    def of_core(array):
        return lax.dynamic_index_in_dim(
            array.reshape(NZ, 2, TOK, 2), core, axis=1, keepdims=False
        )

    named = of_core(routes)
    weights = of_core(token_expert_weights)
    onehot = (named[..., None] == jnp.arange(NSP, dtype=jnp.int32)).astype(F32)
    earlier = jnp.tril(jnp.ones((TOK, TOK), F32), -1)
    ahead = jnp.einsum("ij,zje->zie", earlier, jnp.sum(onehot, axis=2))
    position = jnp.sum(ahead[:, :, None, :] * onehot, axis=3)
    base = named.astype(F32) * SLOT + position
    shift = CAP * jnp.arange(GROUPS, dtype=F32)
    places = base[:, None] + shift[None, :, None, None]
    table = jnp.concatenate(
        [places, jnp.broadcast_to(weights[:, None], places.shape)], axis=3
    ).reshape(NZ, TROWS, 4)
    row_table = lax.dynamic_index_in_dim(table, z, axis=0, keepdims=False)[:, :2].T
    row_table = jnp.pad(row_table, ((0, 6), (0, 0)), constant_values=-1.0)

    n = jnp.arange(ROWS, dtype=jnp.int32)
    per = ROWS // GROUPS
    inward = (n % per) // CAP * SLOT + n // per * CAP + n % CAP
    outward = (n % SLOT) // CAP * per + n // SLOT * CAP + n % CAP
    perms = jnp.stack([inward, outward], axis=1)

    vmem = pl.BlockSpec(memory_space=pltpu.VMEM)
    hbm = pl.BlockSpec(memory_space=pltpu.HBM)
    dma = pltpu.SemaphoreType.DMA
    width = GROUPS * WIDE
    return pl.pallas_call(
        kernel,
        name="layer",
        out_shape=jax.ShapeDtypeStruct((TOK, width), BF16),
        in_specs=[vmem] * 13 + [hbm] * 4,
        out_specs=vmem,
        scratch_shapes=[
            pltpu.VMEM((2, HEAD_DIM, width), BF16),
            pltpu.VMEM((4, width, HEAD_DIM), BF16),
            pltpu.VMEM((2, HEAD_DIM, width), BF16),
            pltpu.VMEM((HEAD_DIM + 8, HEAD_DIM), F32),
            pltpu.VMEM((NSP, HEAD_DIM + 8, HEAD_DIM), F32),
            pltpu.VMEM((NSP, 8, HEAD_DIM), F32),
            pltpu.VMEM((LEN, HEAD_DIM), F32),
            pltpu.VMEM((LEN, HEAD_DIM), F32),
            pltpu.VMEM((LEN // 2, HEAD_DIM), F32),
            pltpu.VMEM((LEN // 2, HEAD_DIM), F32),
            pltpu.VMEM((LEN // 2, HEAD_DIM), BF16),
            pltpu.VMEM((LEN // 2, HEAD_DIM), BF16),
            pltpu.VMEM((NZ, TROWS, WIDE), F32),
            pltpu.VMEM((NZ, TROWS, WIDE), BF16),
            pltpu.VMEM((NZ + 1, TROWS, WIDE), BF16),
            pltpu.VMEM((TROWS, WIDE), BF16),
            pltpu.VMEM((TROWS, WIDE), BF16),
            pltpu.VMEM((ROWS, WIDE), BF16),
            pltpu.VMEM((ROWS, WIDE), BF16),
            pltpu.VMEM((ROWS, ROWS), BF16),
            pltpu.VMEM((ROWS, ROWS), BF16),
            pltpu.VMEM((NZ, ROWS, WIDE), BF16),
            pltpu.VMEM((ROWS, WIDE), BF16),
            pltpu.VMEM((NZ, ROWS, WIDE), BF16),
            pltpu.VMEM((NZ, ROWS, WIDE), BF16),
            pltpu.VMEM((NZ, TROWS, WIDE), BF16),
            pltpu.VMEM((NZ + 1, TROWS, WIDE), BF16),
            pltpu.VMEM((TROWS, WIDE), F32),
            dma((4,)), dma((4,)), dma((4,)), dma((NSP,)), dma((NSP,)), dma((2,)),
            dma((NZ, PIECES)), dma((NZ + 1, PIECES)),
            dma((2,)), dma((NZ - 1, PIECES)), dma((NZ - 1, PIECES)),
            dma((NZ,)), dma((NZ,)), dma((NZ,)), dma((NZ + 1,)),
        ],
        compiler_params=pltpu.CompilerParams(
            collective_id=0, has_side_effects=True, vmem_limit_bytes=60 << 20
        ),
    )(
        queries,
        cell_key_rows,
        cell_value_rows,
        output_gate_logits,
        input_gate_logs,
        forget_gate_logits,
        extra_log_forget,
        head_norm_gain.reshape(1, HEAD_DIM),
        resid,
        expert_norm_gain.reshape(GROUPS, WIDE),
        table,
        row_table,
        perms,
        cell_output_matrix,
        expert_gate_matrix[0],
        expert_up_matrix[0],
        expert_down_matrix[0],
    )


def solution(mesh):
    in_specs = (
        P("sp", "tp"),
        P("sp", "tp"),
        P("sp", "tp"),
        P("sp", "tp"),
        P("tp", "sp"),
        P("tp", "sp"),
        P("tp", "sp"),
        P("tp"),
        P("tp", None),
        P("sp", None),
        P(),
        P("sp", None),
        P("sp", None),
        P("sp", None, "tp"),
        P("sp", None, "tp"),
        P("sp", "tp", None),
    )
    return jax.shard_map(
        local, mesh=mesh, in_specs=in_specs, out_specs=P(("sp", "tp"), None), check_vma=False
    )
```

```python
import jax
import jax.numpy as jnp
from jax import lax
from jax.experimental import pallas as pl
from jax.experimental.pallas import tpu as pltpu
from jax.sharding import PartitionSpec as P

MESH = pl.DeviceIdType.MESH
F32 = jnp.float32
BF16 = jnp.bfloat16

HEAD_DIM = 128
NSP = 16
NZ = 8
LEN = 384
TOK = 24
CAP = 6
GROUPS = 16
WIDE = 256
TURNS = 2
GT = GROUPS // TURNS
SLOT = GT * CAP
ROWS = NSP * SLOT
TROWS = GROUPS * TOK
HROWS = GT * TOK
PER = ROWS // GT
NX = 4
PIECES = 2
STRIPES = 4

floor_neg = -1e30
norm_eps = 1e-06


def dot(a, b):
    return jnp.dot(a, b, preferred_element_type=F32)


def two_parts(x):
    high = x.astype(BF16)
    return high, (x - high.astype(F32)).astype(BF16)


def iota(shape, dim):
    return lax.broadcasted_iota(jnp.int32, shape, dim)


def kernel(
    q_ref, k_ref, v_ref, og_ref, ig_ref, fg_ref, ex_ref, hg_ref,
    eng_ref, route_ref, weight_ref,
    resid_hbm, wo_hbm, gate_hbm, up_hbm, down_hbm,
    out_ref,
    wv, gw, dn, resid,
    row_s, tot_send, tot_s, gs, num_s, co_f, co_a, co_b, co_send, co_recv,
    pf, r1_send, r1_recv, am,
    d_send, d_recv, pin, pout, pick, table,
    xring, acc_s, sq_s, ybuf, mixer, t_send, t_recv, r2_send, r2_recv, own,
    load_sem, wx_send, wx_recv, row_ss, row_rs, tot_ss, tot_rs, co_sem, r1_ss, r1_rs,
    d_ss, d_rs, x_ss, x_rs, t_ss, t_rs, r2_ss, r2_rs,
):
    sp = lax.axis_index("sp")
    tp = lax.axis_index("tp")
    core = lax.rem(tp, 2)
    z = tp // 2
    step = jnp.where(core == 0, 1, NZ - 1)
    above = lax.rem(z + 1, NZ) * 2 + core
    below = lax.rem(z + NZ - 1, NZ) * 2 + core
    after = jnp.where(core == 0, above, below)
    mate = z * 2 + 1 - core
    y, x = sp // NX, lax.rem(sp, NX)

    barrier = pltpu.get_barrier_semaphore()

    @pl.loop(1, NSP)
    def _(i):
        pl.semaphore_signal(
            barrier, inc=1, device_id={"sp": lax.rem(sp + i, NSP), "tp": tp}, device_id_type=MESH
        )

    for other in (above, below, mate):
        pl.semaphore_signal(barrier, inc=1, device_id={"sp": sp, "tp": other}, device_id_type=MESH)

    loads = [
        pltpu.make_async_copy(wo_hbm, wv.at[0], load_sem.at[0]),
        pltpu.make_async_copy(gate_hbm, gw.at[0], load_sem.at[1]),
        pltpu.make_async_copy(up_hbm, gw.at[1], load_sem.at[2]),
        pltpu.make_async_copy(down_hbm, dn.at[0], load_sem.at[3]),
        pltpu.make_async_copy(
            resid_hbm.at[pl.ds(pl.multiple_of(tp * TOK, 8), TOK)], resid, load_sem.at[4]
        ),
    ]
    for load in loads:
        load.start()

    tt = iota((LEN, LEN), 0)
    ss = iota((LEN, LEN), 1)
    causal = ss <= tt
    fg = fg_ref[...]
    f_row = jnp.minimum(fg, 0.0) - jnp.log1p(jnp.exp(-jnp.abs(fg))) + ex_ref[...]
    i_row = ig_ref[...]
    f_all = jnp.broadcast_to(f_row, (LEN, LEN))
    f_col = jnp.sum(jnp.where(ss == tt, f_all, 0.0), axis=1, keepdims=True)
    i_col = jnp.sum(
        jnp.where(ss == tt, jnp.broadcast_to(i_row, (LEN, LEN)), 0.0), axis=1, keepdims=True
    )
    c_col = jnp.sum(jnp.where(causal, f_all, 0.0), axis=1, keepdims=True)
    c_row = jnp.sum(
        jnp.where(tt <= ss, jnp.broadcast_to(f_col, (LEN, LEN)), 0.0), axis=0, keepdims=True
    )
    total = jnp.sum(f_row, axis=1, keepdims=True)
    scale = HEAD_DIM ** (-0.5)
    write = i_col + total - c_col
    stab_dev = jnp.max(write, axis=0, keepdims=True)
    kw = k_ref[...].astype(F32) * (jnp.exp(write - stab_dev) * scale)
    kw_h, kw_l = two_parts(kw)
    dims = (((0,), (0,)), ((), ()))
    v = v_ref[...]
    cell_dev = lax.dot_general(kw_h, v, dims, preferred_element_type=F32) + lax.dot_general(
        kw_l, v, dims, preferred_element_type=F32
    )

    def packed(cell, stab, tot):
        numbers = jnp.where(
            iota((8, HEAD_DIM), 0) == 0,
            jnp.broadcast_to(stab, (8, HEAD_DIM)),
            jnp.broadcast_to(tot, (8, HEAD_DIM)),
        )
        return jnp.concatenate([cell, numbers], axis=0)

    row_s[x] = packed(cell_dev, stab_dev, total)
    q = q_ref[...]
    scores = lax.dot_general(
        q, k_ref[...], (((1,), (1,)), ((), ())), preferred_element_type=F32
    ) * scale
    inner = jnp.where(causal, c_col - c_row + i_row, floor_neg)
    top = jnp.max(inner, axis=1, keepdims=True)
    p_h, p_l = two_parts(scores * jnp.exp(inner - top))
    num_s[...] = dot(p_h, v) + dot(p_l, v)

    def part_of(n, size):
        return jnp.floor((n.astype(F32) + 0.5) * (1.0 / size))

    same = part_of(iota((LEN, 1), 0), TOK) == part_of(iota((1, LEN), 1), TOK)
    earlier = jnp.where(same & (tt < ss), 1.0, 0.0).astype(BF16)
    named = [iota((NSP, LEN), 0) == route_ref[i : i + 1, :] for i in range(2)]
    onehot = [jnp.where(n, 1.0, 0.0) for n in named]
    ahead = dot((onehot[0] + onehot[1]).astype(BF16), earlier)
    places = [jnp.sum(ahead * o, axis=0, keepdims=True) for o in onehot]
    line = iota((HEAD_DIM, LEN), 0)
    rows = jnp.zeros((HEAD_DIM, LEN), F32)
    for i in range(2):
        rows = jnp.where(line == i, route_ref[i : i + 1, :].astype(F32) * SLOT + places[i], rows)
        rows = jnp.where(line == i + 2, weight_ref[i : i + 1, :], rows)
    table[...] = jnp.transpose(rows)

    def spots(tokens):
        return [
            jnp.concatenate([tokens[:, i : i + 1] + CAP * j for j in range(GT)], axis=0)
            for i in range(2)
        ]

    def block_rows(block):
        return pl.ds(pl.multiple_of(block * TOK, 8), TOK)

    place = iota((HROWS, ROWS), 1).astype(F32)
    first, second = spots(table[block_rows(tp), :])
    pick[...] = jnp.transpose(
        jnp.where((place == first) | (place == second), 1.0, 0.0)
    ).astype(BF16)

    def reordered(outer, middle):
        n = iota((ROWS, 1), 0)
        a = part_of(n, outer)
        rest = n.astype(F32) - outer * a
        b = jnp.floor((rest + 0.5) * (1.0 / CAP))
        source = b * middle + a * CAP + (rest - CAP * b)
        return jnp.where(iota((ROWS, ROWS), 1).astype(F32) == source, 1.0, 0.0).astype(BF16)

    pin[...] = reordered(PER, SLOT)
    pout[...] = reordered(SLOT, PER)

    pl.semaphore_wait(barrier, NSP - 1 + 3)

    def row_copy_x(i):
        return pltpu.make_async_remote_copy(
            src_ref=row_s.at[x], dst_ref=row_s.at[x], send_sem=row_ss.at[i], recv_sem=row_rs.at[x],
            device_id={"sp": y * NX + lax.rem(x + i, NX), "tp": tp}, device_id_type=MESH,
        )

    def row_arrival(source):
        return pltpu.make_async_remote_copy(
            src_ref=row_s.at[source], dst_ref=row_s.at[source],
            send_sem=row_ss.at[0], recv_sem=row_rs.at[source],
            device_id={"sp": sp, "tp": mate}, device_id_type=MESH,
        )

    def total_row_copy(to, source):
        return pltpu.make_async_remote_copy(
            src_ref=tot_send, dst_ref=tot_s.at[source],
            send_sem=tot_ss.at[to], recv_sem=tot_rs.at[source],
            device_id={"sp": to * NX + x, "tp": tp}, device_id_type=MESH,
        )

    for i in range(1, NX):
        row_copy_x(i).start()

    pairs = [(wo_hbm, wv.at[1]), (gate_hbm, gw.at[2]), (up_hbm, gw.at[3]), (down_hbm, dn.at[1])]
    shared = [
        pltpu.make_async_remote_copy(
            src_ref=source, dst_ref=target, send_sem=wx_send.at[i], recv_sem=wx_recv.at[i],
            device_id={"sp": sp, "tp": mate}, device_id_type=MESH,
        )
        for i, (source, target) in enumerate(pairs)
    ]
    for copy in shared:
        copy.start()

    for i in range(1, NX):
        row_arrival(lax.rem(x + i, NX)).wait_recv()

    low = jnp.full((1, HEAD_DIM), floor_neg, F32)
    none = jnp.zeros((1, HEAD_DIM), F32)
    blank = jnp.zeros((HEAD_DIM, HEAD_DIM), F32)

    def fold(buffer, at, count, carry):
        def one(i, carry):
            top, tot = carry
            n = count - 1 - i
            here = buffer[n, HEAD_DIM : HEAD_DIM + 1, :] + tot
            gs[at + n, 0:1, :] = here
            return jnp.maximum(top, here), tot + buffer[n, HEAD_DIM + 1 : HEAD_DIM + 2, :]

        return lax.fori_loop(0, count, one, carry)

    def weighted(buffer, at, count, stab, cell):
        def one(n, cell):
            return cell + jnp.exp(gs[at + n, 0:1, :] - stab) * buffer[n, :HEAD_DIM, :]

        return lax.fori_loop(0, count, one, cell)

    row_stab, row_tot = fold(row_s, 0, NX, (low, none))
    tot_send[...] = packed(weighted(row_s, 0, NX, row_stab, blank), row_stab, row_tot)

    @pl.loop(y + 1, NX)
    def _(to):
        total_row_copy(to, y).start()

    carry = fold(row_s, 0, x, (low, none))

    @pl.loop(0, y)
    def _(source):
        total_row_copy(source, source).wait_recv()

    stab0, tot0 = fold(tot_s, NX, y, carry)
    start_stab = jnp.maximum(stab0, tot0)
    start_cell = weighted(row_s, 0, x, start_stab, blank)
    cell_h, cell_l = two_parts(weighted(tot_s, NX, y, start_stab, start_cell))
    carried = c_col + start_stab[:, 0:1]
    stab = jnp.maximum(top, carried)
    numer = jnp.exp(top - stab) * num_s[...] + jnp.exp(carried - stab) * (
        dot(q, cell_h) + dot(q, cell_l)
    )
    scaled = (
        numer
        * lax.rsqrt(jnp.mean(numer * numer, axis=1, keepdims=True) + norm_eps)
        * hg_ref[...]
    )
    co_f[...] = scaled / (1.0 + jnp.exp(-og_ref[...].astype(F32)))
    for i in range(NZ):
        mine = pl.multiple_of((2 * i + core) * TOK, 8)
        theirs = pl.multiple_of((2 * i + 1 - core) * TOK, 8)
        co_a[i * TOK : (i + 1) * TOK, :] = co_f[pl.ds(mine, TOK), :]
        co_b[i * TOK : (i + 1) * TOK, :] = co_f[pl.ds(theirs, TOK), :]
    co_send[...] = co_b[...].astype(BF16)
    swap = pltpu.make_async_remote_copy(
        src_ref=co_send, dst_ref=co_recv, send_sem=co_sem.at[0], recv_sem=co_sem.at[1],
        device_id={"sp": sp, "tp": mate}, device_id_type=MESH,
    )
    swap.start()
    mine_b = co_a[...].astype(BF16)

    for i in range(1, NX):
        row_copy_x(i).wait_send()

    @pl.loop(y + 1, NX)
    def _(to):
        total_row_copy(to, y).wait_send()

    loads[0].wait()
    shared[0].wait()
    swap.wait()
    both = jnp.concatenate([mine_b, co_recv[...]], axis=1)

    @pl.loop(0, GROUPS)
    def _(j):
        at = pl.ds(pl.multiple_of(j * WIDE, WIDE), WIDE)
        part = dot(both, wv[:, :, at].reshape(2 * HEAD_DIM, WIDE))
        for i in range(NZ):
            pf[i, pl.ds(pl.multiple_of(j * TOK, 8), TOK), :] = part[i * TOK : (i + 1) * TOK]

    srows = TROWS // STRIPES

    def hops(d, p):
        return 4 if (p % 2 == 0) == (d == 0) else 3

    def sum_copy(d, m, p):
        rows = pl.ds(p * srows, srows)
        return pltpu.make_async_remote_copy(
            src_ref=r1_send.at[d, m, rows], dst_ref=r1_recv.at[d, m, rows],
            send_sem=r1_ss.at[d, m, p], recv_sem=r1_rs.at[d, m, p],
            device_id={"sp": sp, "tp": (above, below)[d]}, device_id_type=MESH,
        )

    def sum_steps(h, m):
        for d in range(2):
            for p in sorted((2 * h, 2 * h + 1), key=lambda p: -hops(d, p)):
                left = hops(d, p) - m
                if left > 0:
                    rows = slice(p * srows, (p + 1) * srows)
                    part = pf[lax.rem(z + (left if d == 0 else NZ - left), NZ), rows]
                    if m > 0:
                        sum_copy(d, m - 1, p).wait_recv()
                        part = part + r1_recv[d, m - 1, rows].astype(F32)
                    r1_send[d, m, rows] = part.astype(BF16)
                    sum_copy(d, m, p).start()

    def slot_rows(s):
        return pl.ds(pl.multiple_of(s * SLOT, SLOT), SLOT)

    def dispatch(h):
        for p in (2 * h, 2 * h + 1):
            rows = slice(p * srows, (p + 1) * srows)
            for d in range(2):
                sum_copy(d, hops(d, p) - 1, p).wait_recv()
            sides = [r1_recv[d, hops(d, p) - 1, rows].astype(F32) for d in range(2)]
            width = srows // TOK
            old = jnp.concatenate(
                [
                    resid[:, j * WIDE : (j + 1) * WIDE].astype(F32)
                    for j in range(p * width, (p + 1) * width)
                ],
                axis=0,
            )
            am[rows] = (old + (pf[z, rows] + sides[0] + sides[1])).astype(BF16)
        d_send[h] = dot(pick[...], am[h * HROWS : (h + 1) * HROWS]).astype(BF16)

        @pl.loop(1, NSP)
        def _(i):
            to = lax.rem(sp + i, NSP)
            pltpu.make_async_remote_copy(
                src_ref=d_send.at[h, slot_rows(to)], dst_ref=d_recv.at[h, slot_rows(sp)],
                send_sem=d_ss.at[h], recv_sem=d_rs.at[h],
                device_id={"sp": to, "tp": tp}, device_id_type=MESH,
            ).start()

        d_recv[h, slot_rows(sp)] = d_send[h, slot_rows(sp)]

    loads[4].wait()
    sum_steps(0, 0)
    for m in range(1, 4):
        sum_steps(0, m)
        sum_steps(1, m - 1)
    dispatch(0)
    sum_steps(1, 3)
    dispatch(1)

    for load in loads[1:4]:
        load.wait()
    for copy in shared[1:]:
        copy.wait()

    others = pl.ds(0, ROWS - SLOT)
    xrows = ROWS // PIECES

    def block_of(k):
        return lax.rem(z + NZ * NZ - step * k, NZ)

    def row_copy(k, h, p):
        rows = pl.ds(pl.multiple_of(p * xrows, xrows), xrows)
        return pltpu.make_async_remote_copy(
            src_ref=xring.at[k, h, rows], dst_ref=xring.at[k + 1, h, rows],
            send_sem=x_ss.at[k, h, p], recv_sem=x_rs.at[k, h, p],
            device_id={"sp": sp, "tp": after}, device_id_type=MESH,
        )

    def total_copy(k, h):
        return pltpu.make_async_remote_copy(
            src_ref=r2_send.at[k, h], dst_ref=r2_recv.at[k + 1, h],
            send_sem=r2_ss.at[k, h], recv_sem=r2_rs.at[k + 1, h],
            device_id={"sp": sp, "tp": after}, device_id_type=MESH,
        )

    def arrive(k, h):
        @pl.when(k == 0)
        def _():
            pltpu.make_async_copy(d_recv.at[h, others], d_recv.at[h, others], d_rs.at[h]).wait()
            xring[0, h] = dot(pin[...], d_recv[h]).astype(BF16)

        @pl.loop(0, PIECES)
        def _(p):
            @pl.when(k > 0)
            def _():
                row_copy(k - 1, h, p).wait_recv()

            @pl.when(k < NZ - 1)
            def _():
                row_copy(k, h, p).start()

    def first_part(k, h):
        acc = jnp.zeros((PER, 4 * HEAD_DIM), F32)
        squares = jnp.zeros((PER, WIDE), F32)
        for j in range(GT):
            at = slice((h * GT + j) * WIDE, (h * GT + j + 1) * WIDE)
            rows = xring[k, h, j * PER : (j + 1) * PER, :].astype(F32)
            squares = squares + rows * rows
            w = jnp.concatenate([gw[i, at, :] for i in range(4)], axis=1)
            acc = acc + dot((rows * eng_ref[:, at]).astype(BF16), w)
        return acc, squares

    def second_part(k, acc, squares):
        mean = jnp.sum(squares, axis=1, keepdims=True) * (1.0 / (GROUPS * WIDE))
        acc = acc * lax.rsqrt(mean + norm_eps)
        acts = []
        for i in range(2):
            gate = acc[:, 2 * i * HEAD_DIM : (2 * i + 1) * HEAD_DIM]
            upper = acc[:, (2 * i + 1) * HEAD_DIM : (2 * i + 2) * HEAD_DIM]
            acts.append((gate / (1.0 + jnp.exp(-gate)) * upper).astype(BF16))
        act = jnp.concatenate(acts, axis=1)
        for h in range(TURNS):
            for j in range(GT):
                at = slice((h * GT + j) * WIDE, (h * GT + j + 1) * WIDE)
                w = dn[:, :, at].reshape(2 * HEAD_DIM, WIDE)
                ybuf[h, j * PER : (j + 1) * PER, :] = dot(act, w).astype(BF16)
            t_send[k, h] = dot(pout[...], ybuf[h]).astype(BF16)

            @pl.loop(1, NSP)
            def _(i, h=h):
                to = lax.rem(sp + i, NSP)
                pltpu.make_async_remote_copy(
                    src_ref=t_send.at[k, h, slot_rows(to)], dst_ref=t_recv.at[k, h, slot_rows(sp)],
                    send_sem=t_ss.at[k, h], recv_sem=t_rs.at[k, h],
                    device_id={"sp": to, "tp": tp}, device_id_type=MESH,
                ).start()

            t_recv[k, h, slot_rows(sp)] = t_send[k, h, slot_rows(sp)]

    def combine(k, h):
        if h == 0:
            tokens = table[block_rows(block_of(k) * 2 + core), :]
            first, second = spots(tokens)
            weights = [jnp.concatenate([tokens[:, i : i + 1]] * GT, axis=0) for i in (2, 3)]
            place = iota((HROWS, ROWS), 1).astype(F32)
            weight = jnp.where(place == first, weights[0], 0.0) + jnp.where(
                place == second, weights[1], 0.0
            )
            w_h, w_l = two_parts(weight)
            mixer[:HROWS] = w_h
            mixer[HROWS:] = w_l
        pltpu.make_async_copy(
            t_recv.at[k, h, others], t_recv.at[k, h, others], t_rs.at[k, h]
        ).wait()
        mixed = dot(mixer[...], t_recv[k, h])
        mixed = mixed[:HROWS] + mixed[HROWS:]

        @pl.when(k == 0)
        def _():
            own[h] = mixed

        @pl.when(k == 1)
        def _():
            r2_send[k, h] = mixed.astype(BF16)
            total_copy(k, h).start()

        @pl.when(k > 1)
        def _():
            total_copy(k - 1, h).wait_recv()
            r2_send[k, h] = (mixed + r2_recv[k, h].astype(F32)).astype(BF16)
            total_copy(k, h).start()

    @pl.loop(0, NZ)
    def _(k):
        arrive(k, 0)
        acc, squares = first_part(k, 0)
        acc_s[...] = acc
        sq_s[...] = squares

        @pl.when(k > 0)
        def _():
            combine(k - 1, 0)

        arrive(k, 1)
        acc, squares = first_part(k, 1)
        second_part(k, acc_s[...] + acc, sq_s[...] + squares)

        @pl.when(k > 0)
        def _():
            combine(k - 1, 1)

    for h in range(TURNS):
        combine(NZ - 1, h)
    for h in range(TURNS):
        total_copy(NZ - 1, h).wait_recv()
        result = am[h * HROWS : (h + 1) * HROWS].astype(F32) + (
            own[h] + r2_recv[NZ, h].astype(F32)
        )
        for j in range(GT):
            at = slice((h * GT + j) * WIDE, (h * GT + j + 1) * WIDE)
            out_ref[:, at] = result[j * TOK : (j + 1) * TOK].astype(BF16)

    for d in range(2):
        for p in range(STRIPES):
            for m in range(hops(d, p)):
                sum_copy(d, m, p).wait_send()

    @pl.loop(1, NZ)
    def _(k):
        @pl.loop(0, TURNS)
        def _(h):
            total_copy(k, h).wait_send()

            @pl.loop(0, PIECES)
            def _(p):
                row_copy(k - 1, h, p).wait_send()

    @pl.loop(0, TURNS)
    def _(h):
        pltpu.make_async_copy(d_send.at[h, others], d_send.at[h, others], d_ss.at[h]).wait()

        @pl.loop(0, NZ)
        def _(k):
            pltpu.make_async_copy(
                t_send.at[k, h, others], t_send.at[k, h, others], t_ss.at[k, h]
            ).wait()


def local(
    queries,
    cell_key_rows,
    cell_value_rows,
    output_gate_logits,
    input_gate_logs,
    forget_gate_logits,
    extra_log_forget,
    head_norm_gain,
    cell_output_matrix,
    residual,
    expert_norm_gain,
    routes,
    token_expert_weights,
    expert_gate_matrix,
    expert_up_matrix,
    expert_down_matrix,
):
    vmem = pl.BlockSpec(memory_space=pltpu.VMEM)
    hbm = pl.BlockSpec(memory_space=pltpu.HBM)
    dma = pltpu.SemaphoreType.DMA
    width = GROUPS * WIDE
    return pl.pallas_call(
        kernel,
        name="layer",
        out_shape=jax.ShapeDtypeStruct((TOK, width), BF16),
        in_specs=[vmem] * 11 + [hbm] * 5,
        out_specs=vmem,
        scratch_shapes=[
            pltpu.VMEM((2, HEAD_DIM, width), BF16),
            pltpu.VMEM((4, width, HEAD_DIM), BF16),
            pltpu.VMEM((2, HEAD_DIM, width), BF16),
            pltpu.VMEM((TOK, width), BF16),
            pltpu.VMEM((NX, HEAD_DIM + 8, HEAD_DIM), F32),
            pltpu.VMEM((HEAD_DIM + 8, HEAD_DIM), F32),
            pltpu.VMEM((NX, HEAD_DIM + 8, HEAD_DIM), F32),
            pltpu.VMEM((NSP, 8, HEAD_DIM), F32),
            pltpu.VMEM((LEN, HEAD_DIM), F32),
            pltpu.VMEM((LEN, HEAD_DIM), F32),
            pltpu.VMEM((LEN // 2, HEAD_DIM), F32),
            pltpu.VMEM((LEN // 2, HEAD_DIM), F32),
            pltpu.VMEM((LEN // 2, HEAD_DIM), BF16),
            pltpu.VMEM((LEN // 2, HEAD_DIM), BF16),
            pltpu.VMEM((NZ, TROWS, WIDE), F32),
            pltpu.VMEM((2, 4, TROWS, WIDE), BF16),
            pltpu.VMEM((2, 4, TROWS, WIDE), BF16),
            pltpu.VMEM((TROWS, WIDE), BF16),
            pltpu.VMEM((TURNS, ROWS, WIDE), BF16),
            pltpu.VMEM((TURNS, ROWS, WIDE), BF16),
            pltpu.VMEM((ROWS, ROWS), BF16),
            pltpu.VMEM((ROWS, ROWS), BF16),
            pltpu.VMEM((ROWS, HROWS), BF16),
            pltpu.VMEM((LEN, HEAD_DIM), F32),
            pltpu.VMEM((NZ, TURNS, ROWS, WIDE), BF16),
            pltpu.VMEM((PER, 4 * HEAD_DIM), F32),
            pltpu.VMEM((PER, WIDE), F32),
            pltpu.VMEM((TURNS, ROWS, WIDE), BF16),
            pltpu.VMEM((2 * HROWS, ROWS), BF16),
            pltpu.VMEM((NZ, TURNS, ROWS, WIDE), BF16),
            pltpu.VMEM((NZ, TURNS, ROWS, WIDE), BF16),
            pltpu.VMEM((NZ, TURNS, HROWS, WIDE), BF16),
            pltpu.VMEM((NZ + 1, TURNS, HROWS, WIDE), BF16),
            pltpu.VMEM((TURNS, HROWS, WIDE), F32),
            dma((5,)), dma((4,)), dma((4,)), dma((NX,)), dma((NX,)), dma((NX,)), dma((NX,)), dma((2,)),
            dma((2, 4, STRIPES)), dma((2, 4, STRIPES)),
            dma((TURNS,)), dma((TURNS,)),
            dma((NZ - 1, TURNS, PIECES)), dma((NZ - 1, TURNS, PIECES)),
            dma((NZ, TURNS)), dma((NZ, TURNS)), dma((NZ, TURNS)), dma((NZ + 1, TURNS)),
        ],
        compiler_params=pltpu.CompilerParams(
            collective_id=0, has_side_effects=True, vmem_limit_bytes=60 << 20
        ),
    )(
        queries,
        cell_key_rows,
        cell_value_rows,
        output_gate_logits,
        input_gate_logs,
        forget_gate_logits,
        extra_log_forget,
        head_norm_gain.reshape(1, HEAD_DIM),
        expert_norm_gain.reshape(1, width),
        routes.T,
        token_expert_weights.T,
        residual,
        cell_output_matrix,
        expert_gate_matrix[0],
        expert_up_matrix[0],
        expert_down_matrix[0],
    )


def solution(mesh):
    in_specs = (
        P("sp", "tp"),
        P("sp", "tp"),
        P("sp", "tp"),
        P("sp", "tp"),
        P("tp", "sp"),
        P("tp", "sp"),
        P("tp", "sp"),
        P("tp"),
        P("tp", None),
        P("sp", None),
        P(),
        P("sp", None),
        P("sp", None),
        P("sp", None, "tp"),
        P("sp", None, "tp"),
        P("sp", "tp", None),
    )
    return jax.shard_map(
        local, mesh=mesh, in_specs=in_specs, out_specs=P(("sp", "tp"), None), check_vma=False
    )
```

```python
import jax
import jax.numpy as jnp
from jax import lax
from jax.experimental import pallas as pl
from jax.experimental.pallas import tpu as pltpu
from jax.sharding import PartitionSpec as P

MESH = pl.DeviceIdType.MESH
F32 = jnp.float32
BF16 = jnp.bfloat16

HEAD_DIM = 128
NSP = 16
NZ = 8
LEN = 384
TOK = 24
CAP = 6
GROUPS = 16
WIDE = 256
TURNS = 2
GT = GROUPS // TURNS
SLOT = GT * CAP
ROWS = NSP * SLOT
TROWS = GROUPS * TOK
HROWS = GT * TOK
PER = ROWS // GT
NX = 4
PIECES = 2
STRIPES = 4

floor_neg = -1e30
norm_eps = 1e-06


def dot(a, b):
    return jnp.dot(a, b, preferred_element_type=F32)


def two_parts(x):
    high = x.astype(BF16)
    return high, (x - high.astype(F32)).astype(BF16)


def iota(shape, dim):
    return lax.broadcasted_iota(jnp.int32, shape, dim)


def kernel(
    q_ref, k_ref, v_ref, og_ref, ig_ref, fg_ref, ex_ref, hg_ref,
    eng_ref, route_ref, weight_ref,
    resid_hbm, wo_hbm, gate_hbm, up_hbm, down_hbm,
    out_ref,
    wv, gw, dn, resid,
    row_s, tot_send, tot_s, gs, num_s, co_f, co_a, co_b, co_send, co_recv,
    pf, r1_send, r1_recv, am,
    d_send, d_recv, e_send, e_recv, am_next, pin, pout, pick, pick_next, table,
    xring, acc_s, sq_s, ybuf, mixer, t_send, t_recv, r2_send, r2_recv, own, l_send, l_recv,
    load_sem, wx_send, wx_recv, row_ss, row_rs, tot_ss, tot_rs, co_sem, r1_ss, r1_rs,
    d_ss, d_rs, e_ss, e_rs, a_ss, a_rs, l_ss, l_rs, x_ss, x_rs, t_ss, t_rs, r2_ss, r2_rs,
):
    sp = lax.axis_index("sp")
    tp = lax.axis_index("tp")
    core = lax.rem(tp, 2)
    z = tp // 2
    step = jnp.where(core == 0, 1, NZ - 1)
    above = lax.rem(z + 1, NZ) * 2 + core
    below = lax.rem(z + NZ - 1, NZ) * 2 + core
    after = jnp.where(core == 0, above, below)
    before = jnp.where(core == 0, below, above)
    second_after = lax.rem(z + 2 * step, NZ) * 2 + core
    second_before = lax.rem(z + 2 * (NZ - step), NZ) * 2 + core
    mate = z * 2 + 1 - core
    y, x = sp // NX, lax.rem(sp, NX)

    barrier = pltpu.get_barrier_semaphore()

    @pl.loop(1, NSP)
    def _(i):
        pl.semaphore_signal(
            barrier, inc=1, device_id={"sp": lax.rem(sp + i, NSP), "tp": tp}, device_id_type=MESH
        )

    for other in (above, below, mate, second_after, second_before):
        pl.semaphore_signal(barrier, inc=1, device_id={"sp": sp, "tp": other}, device_id_type=MESH)

    loads = [
        pltpu.make_async_copy(wo_hbm, wv.at[0], load_sem.at[0]),
        pltpu.make_async_copy(gate_hbm, gw.at[0], load_sem.at[1]),
        pltpu.make_async_copy(up_hbm, gw.at[1], load_sem.at[2]),
        pltpu.make_async_copy(down_hbm, dn.at[0], load_sem.at[3]),
        pltpu.make_async_copy(
            resid_hbm.at[pl.ds(pl.multiple_of(tp * TOK, 8), TOK)], resid, load_sem.at[4]
        ),
    ]
    for load in loads:
        load.start()

    tt = iota((LEN, LEN), 0)
    ss = iota((LEN, LEN), 1)
    causal = ss <= tt
    fg = fg_ref[...]
    f_row = jnp.minimum(fg, 0.0) - jnp.log1p(jnp.exp(-jnp.abs(fg))) + ex_ref[...]
    i_row = ig_ref[...]
    f_all = jnp.broadcast_to(f_row, (LEN, LEN))
    f_col = jnp.sum(jnp.where(ss == tt, f_all, 0.0), axis=1, keepdims=True)
    i_col = jnp.sum(
        jnp.where(ss == tt, jnp.broadcast_to(i_row, (LEN, LEN)), 0.0), axis=1, keepdims=True
    )
    c_col = jnp.sum(jnp.where(causal, f_all, 0.0), axis=1, keepdims=True)
    c_row = jnp.sum(
        jnp.where(tt <= ss, jnp.broadcast_to(f_col, (LEN, LEN)), 0.0), axis=0, keepdims=True
    )
    total = jnp.sum(f_row, axis=1, keepdims=True)
    scale = HEAD_DIM ** (-0.5)
    write = i_col + total - c_col
    stab_dev = jnp.max(write, axis=0, keepdims=True)
    kw = k_ref[...].astype(F32) * (jnp.exp(write - stab_dev) * scale)
    kw_h, kw_l = two_parts(kw)
    dims = (((0,), (0,)), ((), ()))
    v = v_ref[...]
    cell_dev = lax.dot_general(kw_h, v, dims, preferred_element_type=F32) + lax.dot_general(
        kw_l, v, dims, preferred_element_type=F32
    )

    def packed(cell, stab, tot):
        numbers = jnp.where(
            iota((8, HEAD_DIM), 0) == 0,
            jnp.broadcast_to(stab, (8, HEAD_DIM)),
            jnp.broadcast_to(tot, (8, HEAD_DIM)),
        )
        return jnp.concatenate([cell, numbers], axis=0)

    row_s[x] = packed(cell_dev, stab_dev, total)
    q = q_ref[...]
    scores = lax.dot_general(
        q, k_ref[...], (((1,), (1,)), ((), ())), preferred_element_type=F32
    ) * scale
    inner = jnp.where(causal, c_col - c_row + i_row, floor_neg)
    top = jnp.max(inner, axis=1, keepdims=True)
    p_h, p_l = two_parts(scores * jnp.exp(inner - top))
    num_s[...] = dot(p_h, v) + dot(p_l, v)

    def part_of(n, size):
        return jnp.floor((n.astype(F32) + 0.5) * (1.0 / size))

    same = part_of(iota((LEN, 1), 0), TOK) == part_of(iota((1, LEN), 1), TOK)
    earlier = jnp.where(same & (tt < ss), 1.0, 0.0).astype(BF16)
    named = [iota((NSP, LEN), 0) == route_ref[i : i + 1, :] for i in range(2)]
    onehot = [jnp.where(n, 1.0, 0.0) for n in named]
    ahead = dot((onehot[0] + onehot[1]).astype(BF16), earlier)
    places = [jnp.sum(ahead * o, axis=0, keepdims=True) for o in onehot]
    line = iota((HEAD_DIM, LEN), 0)
    rows = jnp.zeros((HEAD_DIM, LEN), F32)
    for i in range(2):
        rows = jnp.where(line == i, route_ref[i : i + 1, :].astype(F32) * SLOT + places[i], rows)
        rows = jnp.where(line == i + 2, weight_ref[i : i + 1, :], rows)
    table[...] = jnp.transpose(rows)

    def spots(tokens):
        return [
            jnp.concatenate([tokens[:, i : i + 1] + CAP * j for j in range(GT)], axis=0)
            for i in range(2)
        ]

    def block_rows(block):
        return pl.ds(pl.multiple_of(block * TOK, 8), TOK)

    place = iota((HROWS, ROWS), 1).astype(F32)
    for target, block in ((pick, tp), (pick_next, after)):
        first, second = spots(table[block_rows(block), :])
        target[...] = jnp.transpose(
            jnp.where((place == first) | (place == second), 1.0, 0.0)
        ).astype(BF16)

    def reordered(outer, middle):
        n = iota((ROWS, 1), 0)
        a = part_of(n, outer)
        rest = n.astype(F32) - outer * a
        b = jnp.floor((rest + 0.5) * (1.0 / CAP))
        source = b * middle + a * CAP + (rest - CAP * b)
        return jnp.where(iota((ROWS, ROWS), 1).astype(F32) == source, 1.0, 0.0).astype(BF16)

    pin[...] = reordered(PER, SLOT)
    pout[...] = reordered(SLOT, PER)

    pl.semaphore_wait(barrier, NSP - 1 + 5)

    def row_copy_x(i):
        return pltpu.make_async_remote_copy(
            src_ref=row_s.at[x], dst_ref=row_s.at[x], send_sem=row_ss.at[i], recv_sem=row_rs.at[x],
            device_id={"sp": y * NX + lax.rem(x + i, NX), "tp": tp}, device_id_type=MESH,
        )

    def row_arrival(source):
        return pltpu.make_async_remote_copy(
            src_ref=row_s.at[source], dst_ref=row_s.at[source],
            send_sem=row_ss.at[0], recv_sem=row_rs.at[source],
            device_id={"sp": sp, "tp": mate}, device_id_type=MESH,
        )

    def total_row_copy(to, source):
        return pltpu.make_async_remote_copy(
            src_ref=tot_send, dst_ref=tot_s.at[source],
            send_sem=tot_ss.at[to], recv_sem=tot_rs.at[source],
            device_id={"sp": to * NX + x, "tp": tp}, device_id_type=MESH,
        )

    for i in range(1, NX):
        row_copy_x(i).start()

    pairs = [(wo_hbm, wv.at[1]), (gate_hbm, gw.at[2]), (up_hbm, gw.at[3]), (down_hbm, dn.at[1])]
    shared = [
        pltpu.make_async_remote_copy(
            src_ref=source, dst_ref=target, send_sem=wx_send.at[i], recv_sem=wx_recv.at[i],
            device_id={"sp": sp, "tp": mate}, device_id_type=MESH,
        )
        for i, (source, target) in enumerate(pairs)
    ]
    for copy in shared:
        copy.start()

    for i in range(1, NX):
        row_arrival(lax.rem(x + i, NX)).wait_recv()

    low = jnp.full((1, HEAD_DIM), floor_neg, F32)
    none = jnp.zeros((1, HEAD_DIM), F32)
    blank = jnp.zeros((HEAD_DIM, HEAD_DIM), F32)

    def fold(buffer, at, count, carry):
        def one(i, carry):
            top, tot = carry
            n = count - 1 - i
            here = buffer[n, HEAD_DIM : HEAD_DIM + 1, :] + tot
            gs[at + n, 0:1, :] = here
            return jnp.maximum(top, here), tot + buffer[n, HEAD_DIM + 1 : HEAD_DIM + 2, :]

        return lax.fori_loop(0, count, one, carry)

    def weighted(buffer, at, count, stab, cell):
        def one(n, cell):
            return cell + jnp.exp(gs[at + n, 0:1, :] - stab) * buffer[n, :HEAD_DIM, :]

        return lax.fori_loop(0, count, one, cell)

    row_stab, row_tot = fold(row_s, 0, NX, (low, none))
    tot_send[...] = packed(weighted(row_s, 0, NX, row_stab, blank), row_stab, row_tot)

    @pl.loop(y + 1, NX)
    def _(to):
        total_row_copy(to, y).start()

    carry = fold(row_s, 0, x, (low, none))

    @pl.loop(0, y)
    def _(source):
        total_row_copy(source, source).wait_recv()

    stab0, tot0 = fold(tot_s, NX, y, carry)
    start_stab = jnp.maximum(stab0, tot0)
    start_cell = weighted(row_s, 0, x, start_stab, blank)
    cell_h, cell_l = two_parts(weighted(tot_s, NX, y, start_stab, start_cell))
    carried = c_col + start_stab[:, 0:1]
    stab = jnp.maximum(top, carried)
    numer = jnp.exp(top - stab) * num_s[...] + jnp.exp(carried - stab) * (
        dot(q, cell_h) + dot(q, cell_l)
    )
    scaled = (
        numer
        * lax.rsqrt(jnp.mean(numer * numer, axis=1, keepdims=True) + norm_eps)
        * hg_ref[...]
    )
    co_f[...] = scaled / (1.0 + jnp.exp(-og_ref[...].astype(F32)))
    for i in range(NZ):
        mine = pl.multiple_of((2 * i + core) * TOK, 8)
        theirs = pl.multiple_of((2 * i + 1 - core) * TOK, 8)
        co_a[i * TOK : (i + 1) * TOK, :] = co_f[pl.ds(mine, TOK), :]
        co_b[i * TOK : (i + 1) * TOK, :] = co_f[pl.ds(theirs, TOK), :]
    co_send[...] = co_b[...].astype(BF16)
    swap = pltpu.make_async_remote_copy(
        src_ref=co_send, dst_ref=co_recv, send_sem=co_sem.at[0], recv_sem=co_sem.at[1],
        device_id={"sp": sp, "tp": mate}, device_id_type=MESH,
    )
    swap.start()
    mine_b = co_a[...].astype(BF16)

    for i in range(1, NX):
        row_copy_x(i).wait_send()

    @pl.loop(y + 1, NX)
    def _(to):
        total_row_copy(to, y).wait_send()

    loads[0].wait()
    shared[0].wait()
    swap.wait()
    both = jnp.concatenate([mine_b, co_recv[...]], axis=1)

    def project(h):
        @pl.loop(h * GT, (h + 1) * GT)
        def _(j):
            at = pl.ds(pl.multiple_of(j * WIDE, WIDE), WIDE)
            part = dot(both, wv[:, :, at].reshape(2 * HEAD_DIM, WIDE))
            for i in range(NZ):
                pf[i, pl.ds(pl.multiple_of(j * TOK, 8), TOK), :] = part[i * TOK : (i + 1) * TOK]

    srows = TROWS // STRIPES

    def hops(d, p):
        return 4 if (p % 2 == 0) == (d == 0) else 3

    def sum_copy(d, m, p):
        rows = pl.ds(p * srows, srows)
        return pltpu.make_async_remote_copy(
            src_ref=r1_send.at[d, m, rows], dst_ref=r1_recv.at[d, m, rows],
            send_sem=r1_ss.at[d, m, p], recv_sem=r1_rs.at[d, m, p],
            device_id={"sp": sp, "tp": (above, below)[d]}, device_id_type=MESH,
        )

    def sum_steps(h, m):
        for d in range(2):
            for p in sorted((2 * h, 2 * h + 1), key=lambda p: -hops(d, p)):
                left = hops(d, p) - m
                if left > 0:
                    rows = slice(p * srows, (p + 1) * srows)
                    part = pf[lax.rem(z + (left if d == 0 else NZ - left), NZ), rows]
                    if m > 0:
                        sum_copy(d, m - 1, p).wait_recv()
                        part = part + r1_recv[d, m - 1, rows].astype(F32)
                    r1_send[d, m, rows] = part.astype(BF16)
                    sum_copy(d, m, p).start()

    def slot_rows(s):
        return pl.ds(pl.multiple_of(s * SLOT, SLOT), SLOT)

    def to_experts(h, chosen, tokens, sent, received, send_sem, recv_sem):
        sent[h] = dot(chosen[...], tokens[h * HROWS : (h + 1) * HROWS]).astype(BF16)

        @pl.loop(1, NSP)
        def _(i):
            to = lax.rem(sp + i, NSP)
            pltpu.make_async_remote_copy(
                src_ref=sent.at[h, slot_rows(to)], dst_ref=received.at[h, slot_rows(sp)],
                send_sem=send_sem.at[h], recv_sem=recv_sem.at[h],
                device_id={"sp": to, "tp": tp}, device_id_type=MESH,
            ).start()

        received[h, slot_rows(sp)] = sent[h, slot_rows(sp)]

    def next_copy(h):
        rows = pl.ds(h * HROWS, HROWS)
        return pltpu.make_async_remote_copy(
            src_ref=am.at[rows], dst_ref=am_next.at[rows], send_sem=a_ss.at[h], recv_sem=a_rs.at[h],
            device_id={"sp": sp, "tp": before}, device_id_type=MESH,
        )

    def dispatch(h):
        for p in (2 * h, 2 * h + 1):
            rows = slice(p * srows, (p + 1) * srows)
            for d in range(2):
                sum_copy(d, hops(d, p) - 1, p).wait_recv()
            sides = [r1_recv[d, hops(d, p) - 1, rows].astype(F32) for d in range(2)]
            width = srows // TOK
            old = jnp.concatenate(
                [
                    resid[:, j * WIDE : (j + 1) * WIDE].astype(F32)
                    for j in range(p * width, (p + 1) * width)
                ],
                axis=0,
            )
            am[rows] = (old + (pf[z, rows] + sides[0] + sides[1])).astype(BF16)
        next_copy(h).start()
        to_experts(h, pick, am, d_send, d_recv, d_ss, d_rs)

    def relay(h):
        next_copy(h).wait_recv()
        to_experts(h, pick_next, am_next, e_send, e_recv, e_ss, e_rs)

    project(0)
    sum_steps(0, 0)
    project(1)
    loads[4].wait()
    for m in range(1, 4):
        sum_steps(0, m)
        sum_steps(1, m - 1)
    dispatch(0)
    sum_steps(1, 3)
    dispatch(1)
    relay(0)

    for load in loads[1:4]:
        load.wait()
    for copy in shared[1:]:
        copy.wait()

    others = pl.ds(0, ROWS - SLOT)
    xrows = ROWS // PIECES

    def block_of(k):
        return lax.rem(z + NZ * NZ - step * k, NZ)

    def row_copy(k, h, p):
        rows = pl.ds(pl.multiple_of(p * xrows, xrows), xrows)
        return pltpu.make_async_remote_copy(
            src_ref=xring.at[k, h, rows], dst_ref=xring.at[k + 1, h, rows],
            send_sem=x_ss.at[k, h, p], recv_sem=x_rs.at[k, h, p],
            device_id={"sp": sp, "tp": after}, device_id_type=MESH,
        )

    def total_copy(k, h):
        return pltpu.make_async_remote_copy(
            src_ref=r2_send.at[k, h], dst_ref=r2_recv.at[k + 1, h],
            send_sem=r2_ss.at[k, h], recv_sem=r2_rs.at[k + 1, h],
            device_id={"sp": sp, "tp": jnp.where(k == NZ - 2, second_after, after)},
            device_id_type=MESH,
        )

    def last_copy(h):
        return pltpu.make_async_remote_copy(
            src_ref=l_send.at[h], dst_ref=l_recv.at[h], send_sem=l_ss.at[h], recv_sem=l_rs.at[h],
            device_id={"sp": sp, "tp": after}, device_id_type=MESH,
        )

    def from_plane(k, h, received, recv_sem):
        pltpu.make_async_copy(received.at[h, others], received.at[h, others], recv_sem.at[h]).wait()
        xring[k, h] = dot(pin[...], received[h]).astype(BF16)

    def arrive(t, h):
        k = jnp.where(t <= 2, t, t - 1)

        @pl.when(t == 0)
        def _():
            from_plane(0, h, d_recv, d_rs)

        @pl.when(t != 3)
        def _():
            @pl.loop(0, PIECES)
            def _(p):
                @pl.when(k > 0)
                def _():
                    row_copy(k - 1, h, p).wait_recv()

                @pl.when(k < NZ - 2)
                def _():
                    row_copy(k, h, p).start()

        @pl.when(t == 2)
        def _():
            from_plane(NZ - 1, h, e_recv, e_rs)

    def first_part(k, h):
        acc = jnp.zeros((PER, 4 * HEAD_DIM), F32)
        squares = jnp.zeros((PER, WIDE), F32)
        for j in range(GT):
            at = slice((h * GT + j) * WIDE, (h * GT + j + 1) * WIDE)
            rows = xring[k, h, j * PER : (j + 1) * PER, :].astype(F32)
            squares = squares + rows * rows
            w = jnp.concatenate([gw[i, at, :] for i in range(4)], axis=1)
            acc = acc + dot((rows * eng_ref[:, at]).astype(BF16), w)
        return acc, squares

    def second_part(k, acc, squares):
        mean = jnp.sum(squares, axis=1, keepdims=True) * (1.0 / (GROUPS * WIDE))
        acc = acc * lax.rsqrt(mean + norm_eps)
        acts = []
        for i in range(2):
            gate = acc[:, 2 * i * HEAD_DIM : (2 * i + 1) * HEAD_DIM]
            upper = acc[:, (2 * i + 1) * HEAD_DIM : (2 * i + 2) * HEAD_DIM]
            acts.append((gate / (1.0 + jnp.exp(-gate)) * upper).astype(BF16))
        act = jnp.concatenate(acts, axis=1)
        for h in range(TURNS):
            for j in range(GT):
                at = slice((h * GT + j) * WIDE, (h * GT + j + 1) * WIDE)
                w = dn[:, :, at].reshape(2 * HEAD_DIM, WIDE)
                ybuf[h, j * PER : (j + 1) * PER, :] = dot(act, w).astype(BF16)
            t_send[k, h] = dot(pout[...], ybuf[h]).astype(BF16)

            @pl.loop(1, NSP)
            def _(i, h=h):
                to = lax.rem(sp + i, NSP)
                pltpu.make_async_remote_copy(
                    src_ref=t_send.at[k, h, slot_rows(to)], dst_ref=t_recv.at[k, h, slot_rows(sp)],
                    send_sem=t_ss.at[k, h], recv_sem=t_rs.at[k, h],
                    device_id={"sp": to, "tp": tp}, device_id_type=MESH,
                ).start()

            t_recv[k, h, slot_rows(sp)] = t_send[k, h, slot_rows(sp)]

    def combine(k, h):
        if h == 0:
            tokens = table[block_rows(block_of(k) * 2 + core), :]
            first, second = spots(tokens)
            weights = [jnp.concatenate([tokens[:, i : i + 1]] * GT, axis=0) for i in (2, 3)]
            place = iota((HROWS, ROWS), 1).astype(F32)
            weight = jnp.where(place == first, weights[0], 0.0) + jnp.where(
                place == second, weights[1], 0.0
            )
            w_h, w_l = two_parts(weight)
            mixer[:HROWS] = w_h
            mixer[HROWS:] = w_l
        pltpu.make_async_copy(
            t_recv.at[k, h, others], t_recv.at[k, h, others], t_rs.at[k, h]
        ).wait()
        mixed = dot(mixer[...], t_recv[k, h])
        mixed = mixed[:HROWS] + mixed[HROWS:]

        @pl.when(k == 0)
        def _():
            own[h] = mixed

        @pl.when(k == NZ - 1)
        def _():
            l_send[h] = mixed.astype(BF16)
            last_copy(h).start()

        @pl.when(k == 1)
        def _():
            r2_send[k, h] = mixed.astype(BF16)
            total_copy(k, h).start()

        @pl.when((k > 1) & (k < NZ - 1))
        def _():
            total_copy(k - 1, h).wait_recv()
            r2_send[k, h] = (mixed + r2_recv[k, h].astype(F32)).astype(BF16)
            total_copy(k, h).start()

    @pl.loop(0, NZ)
    def _(t):
        k = jnp.where(t < 2, t, jnp.where(t == 2, NZ - 1, t - 1))
        back = jnp.where(t < 4, t - 2, jnp.where(t == 4, NZ - 1, t - 3))
        arrive(t, 0)
        acc, squares = first_part(k, 0)
        acc_s[...] = acc
        sq_s[...] = squares

        @pl.when(t == 0)
        def _():
            relay(1)

        @pl.when(t >= 2)
        def _():
            combine(back, 0)

        arrive(t, 1)
        acc, squares = first_part(k, 1)
        second_part(k, acc_s[...] + acc, sq_s[...] + squares)

        @pl.when(t >= 2)
        def _():
            combine(back, 1)

    @pl.loop(NZ - 3, NZ - 1)
    def _(k):
        for h in range(TURNS):
            combine(k, h)

    for h in range(TURNS):
        last_copy(h).wait_recv()
    for h in range(TURNS):
        total_copy(NZ - 2, h).wait_recv()
        result = am[h * HROWS : (h + 1) * HROWS].astype(F32) + (
            own[h] + l_recv[h].astype(F32) + r2_recv[NZ - 1, h].astype(F32)
        )
        for j in range(GT):
            at = slice((h * GT + j) * WIDE, (h * GT + j + 1) * WIDE)
            out_ref[:, at] = result[j * TOK : (j + 1) * TOK].astype(BF16)

    for d in range(2):
        for p in range(STRIPES):
            for m in range(hops(d, p)):
                sum_copy(d, m, p).wait_send()

    for h in range(TURNS):
        next_copy(h).wait_send()
        last_copy(h).wait_send()
        pltpu.make_async_copy(e_send.at[h, others], e_send.at[h, others], e_ss.at[h]).wait()

    @pl.loop(1, NZ - 1)
    def _(k):
        @pl.loop(0, TURNS)
        def _(h):
            total_copy(k, h).wait_send()

            @pl.loop(0, PIECES)
            def _(p):
                row_copy(k - 1, h, p).wait_send()

    @pl.loop(0, TURNS)
    def _(h):
        pltpu.make_async_copy(d_send.at[h, others], d_send.at[h, others], d_ss.at[h]).wait()

        @pl.loop(0, NZ)
        def _(k):
            pltpu.make_async_copy(
                t_send.at[k, h, others], t_send.at[k, h, others], t_ss.at[k, h]
            ).wait()


def local(
    queries,
    cell_key_rows,
    cell_value_rows,
    output_gate_logits,
    input_gate_logs,
    forget_gate_logits,
    extra_log_forget,
    head_norm_gain,
    cell_output_matrix,
    residual,
    expert_norm_gain,
    routes,
    token_expert_weights,
    expert_gate_matrix,
    expert_up_matrix,
    expert_down_matrix,
):
    vmem = pl.BlockSpec(memory_space=pltpu.VMEM)
    hbm = pl.BlockSpec(memory_space=pltpu.HBM)
    dma = pltpu.SemaphoreType.DMA
    width = GROUPS * WIDE
    return pl.pallas_call(
        kernel,
        name="layer",
        out_shape=jax.ShapeDtypeStruct((TOK, width), BF16),
        in_specs=[vmem] * 11 + [hbm] * 5,
        out_specs=vmem,
        scratch_shapes=[
            pltpu.VMEM((2, HEAD_DIM, width), BF16),
            pltpu.VMEM((4, width, HEAD_DIM), BF16),
            pltpu.VMEM((2, HEAD_DIM, width), BF16),
            pltpu.VMEM((TOK, width), BF16),
            pltpu.VMEM((NX, HEAD_DIM + 8, HEAD_DIM), F32),
            pltpu.VMEM((HEAD_DIM + 8, HEAD_DIM), F32),
            pltpu.VMEM((NX, HEAD_DIM + 8, HEAD_DIM), F32),
            pltpu.VMEM((NSP, 8, HEAD_DIM), F32),
            pltpu.VMEM((LEN, HEAD_DIM), F32),
            pltpu.VMEM((LEN, HEAD_DIM), F32),
            pltpu.VMEM((LEN // 2, HEAD_DIM), F32),
            pltpu.VMEM((LEN // 2, HEAD_DIM), F32),
            pltpu.VMEM((LEN // 2, HEAD_DIM), BF16),
            pltpu.VMEM((LEN // 2, HEAD_DIM), BF16),
            pltpu.VMEM((NZ, TROWS, WIDE), F32),
            pltpu.VMEM((2, 4, TROWS, WIDE), BF16),
            pltpu.VMEM((2, 4, TROWS, WIDE), BF16),
            pltpu.VMEM((TROWS, WIDE), BF16),
            pltpu.VMEM((TURNS, ROWS, WIDE), BF16),
            pltpu.VMEM((TURNS, ROWS, WIDE), BF16),
            pltpu.VMEM((TURNS, ROWS, WIDE), BF16),
            pltpu.VMEM((TURNS, ROWS, WIDE), BF16),
            pltpu.VMEM((TROWS, WIDE), BF16),
            pltpu.VMEM((ROWS, ROWS), BF16),
            pltpu.VMEM((ROWS, ROWS), BF16),
            pltpu.VMEM((ROWS, HROWS), BF16),
            pltpu.VMEM((ROWS, HROWS), BF16),
            pltpu.VMEM((LEN, HEAD_DIM), F32),
            pltpu.VMEM((NZ, TURNS, ROWS, WIDE), BF16),
            pltpu.VMEM((PER, 4 * HEAD_DIM), F32),
            pltpu.VMEM((PER, WIDE), F32),
            pltpu.VMEM((TURNS, ROWS, WIDE), BF16),
            pltpu.VMEM((2 * HROWS, ROWS), BF16),
            pltpu.VMEM((NZ, TURNS, ROWS, WIDE), BF16),
            pltpu.VMEM((NZ, TURNS, ROWS, WIDE), BF16),
            pltpu.VMEM((NZ, TURNS, HROWS, WIDE), BF16),
            pltpu.VMEM((NZ, TURNS, HROWS, WIDE), BF16),
            pltpu.VMEM((TURNS, HROWS, WIDE), F32),
            pltpu.VMEM((TURNS, HROWS, WIDE), BF16),
            pltpu.VMEM((TURNS, HROWS, WIDE), BF16),
            dma((5,)), dma((4,)), dma((4,)), dma((NX,)), dma((NX,)), dma((NX,)), dma((NX,)), dma((2,)),
            dma((2, 4, STRIPES)), dma((2, 4, STRIPES)),
            dma((TURNS,)), dma((TURNS,)), dma((TURNS,)), dma((TURNS,)),
            dma((TURNS,)), dma((TURNS,)), dma((TURNS,)), dma((TURNS,)),
            dma((NZ - 2, TURNS, PIECES)), dma((NZ - 2, TURNS, PIECES)),
            dma((NZ, TURNS)), dma((NZ, TURNS)), dma((NZ, TURNS)), dma((NZ, TURNS)),
        ],
        compiler_params=pltpu.CompilerParams(
            collective_id=0, has_side_effects=True, vmem_limit_bytes=60 << 20
        ),
    )(
        queries,
        cell_key_rows,
        cell_value_rows,
        output_gate_logits,
        input_gate_logs,
        forget_gate_logits,
        extra_log_forget,
        head_norm_gain.reshape(1, HEAD_DIM),
        expert_norm_gain.reshape(1, width),
        routes.T,
        token_expert_weights.T,
        residual,
        cell_output_matrix,
        expert_gate_matrix[0],
        expert_up_matrix[0],
        expert_down_matrix[0],
    )


def solution(mesh):
    in_specs = (
        P("sp", "tp"),
        P("sp", "tp"),
        P("sp", "tp"),
        P("sp", "tp"),
        P("tp", "sp"),
        P("tp", "sp"),
        P("tp", "sp"),
        P("tp"),
        P("tp", None),
        P("sp", None),
        P(),
        P("sp", None),
        P("sp", None),
        P("sp", None, "tp"),
        P("sp", None, "tp"),
        P("sp", "tp", None),
    )
    return jax.shard_map(
        local, mesh=mesh, in_specs=in_specs, out_specs=P(("sp", "tp"), None), check_vma=False
    )
```

```python
import jax
import jax.numpy as jnp
from jax import lax
from jax.experimental import pallas as pl
from jax.experimental.pallas import tpu as pltpu
from jax.sharding import PartitionSpec as P

MESH = pl.DeviceIdType.MESH
F32 = jnp.float32
BF16 = jnp.bfloat16

HEAD_DIM = 128
NSP = 16
NZ = 8
LEN = 384
TOK = 24
CAP = 6
GROUPS = 16
WIDE = 256
TURNS = 2
GT = GROUPS // TURNS
SLOT = GT * CAP
ROWS = NSP * SLOT
TROWS = GROUPS * TOK
HROWS = GT * TOK
PER = ROWS // GT
NX = 4
LAG = 2
PIECES = 2
STRIPES = 4

floor_neg = -1e30
norm_eps = 1e-06


def dot(a, b):
    return jnp.dot(a, b, preferred_element_type=F32)


def two_parts(x):
    high = x.astype(BF16)
    return high, (x - high.astype(F32)).astype(BF16)


def iota(shape, dim):
    return lax.broadcasted_iota(jnp.int32, shape, dim)


def kernel(
    q_ref, k_ref, v_ref, og_ref, ig_ref, fg_ref, ex_ref, hg_ref,
    eng_ref, route_ref, weight_ref,
    resid_hbm, wo_hbm, gate_hbm, up_hbm, down_hbm,
    out_ref,
    wv, gw, dn, resid,
    row_s, tot_send, tot_s, gs, num_s, co_f, co_a, co_b, co_send, co_recv,
    pf, r1_send, r1_recv, am,
    d_send, d_recv, am_next, pin, pout, pick, pick_next, table,
    xring, acc_s, sq_s, ybuf, mixer, t_send, t_recv, r2_send, r2_recv, own,
    load_sem, wx_send, wx_recv, row_ss, row_rs, tot_ss, tot_rs, co_sem, r1_ss, r1_rs,
    d_ss, d_rs, a_sem, x_ss, x_rs, t_ss, t_rs, r2_ss, r2_rs,
):
    sp = lax.axis_index("sp")
    tp = lax.axis_index("tp")
    core = lax.rem(tp, 2)
    z = tp // 2
    step = jnp.where(core == 0, 1, NZ - 1)
    above = lax.rem(z + 1, NZ) * 2 + core
    below = lax.rem(z + NZ - 1, NZ) * 2 + core
    after = jnp.where(core == 0, above, below)
    before = jnp.where(core == 0, below, above)
    mate = z * 2 + 1 - core
    y, x = sp // NX, lax.rem(sp, NX)

    barrier = pltpu.get_barrier_semaphore()

    @pl.loop(1, NSP)
    def _(i):
        pl.semaphore_signal(
            barrier, inc=1, device_id={"sp": lax.rem(sp + i, NSP), "tp": tp}, device_id_type=MESH
        )

    for other in (above, below, mate):
        pl.semaphore_signal(barrier, inc=1, device_id={"sp": sp, "tp": other}, device_id_type=MESH)

    loads = [
        pltpu.make_async_copy(wo_hbm, wv.at[0], load_sem.at[0]),
        pltpu.make_async_copy(gate_hbm, gw.at[0], load_sem.at[1]),
        pltpu.make_async_copy(up_hbm, gw.at[1], load_sem.at[2]),
        pltpu.make_async_copy(down_hbm, dn.at[0], load_sem.at[3]),
        pltpu.make_async_copy(
            resid_hbm.at[pl.ds(pl.multiple_of(tp * TOK, 8), TOK)], resid, load_sem.at[4]
        ),
    ]
    for load in loads:
        load.start()

    tt = iota((LEN, LEN), 0)
    ss = iota((LEN, LEN), 1)
    causal = ss <= tt
    fg = fg_ref[...]
    f_row = jnp.minimum(fg, 0.0) - jnp.log1p(jnp.exp(-jnp.abs(fg))) + ex_ref[...]
    i_row = ig_ref[...]
    f_all = jnp.broadcast_to(f_row, (LEN, LEN))
    f_col = jnp.sum(jnp.where(ss == tt, f_all, 0.0), axis=1, keepdims=True)
    i_col = jnp.sum(
        jnp.where(ss == tt, jnp.broadcast_to(i_row, (LEN, LEN)), 0.0), axis=1, keepdims=True
    )
    c_col = jnp.sum(jnp.where(causal, f_all, 0.0), axis=1, keepdims=True)
    c_row = jnp.sum(
        jnp.where(tt <= ss, jnp.broadcast_to(f_col, (LEN, LEN)), 0.0), axis=0, keepdims=True
    )
    total = jnp.sum(f_row, axis=1, keepdims=True)
    scale = HEAD_DIM ** (-0.5)
    write = i_col + total - c_col
    stab_dev = jnp.max(write, axis=0, keepdims=True)
    kw = k_ref[...].astype(F32) * (jnp.exp(write - stab_dev) * scale)
    kw_h, kw_l = two_parts(kw)
    dims = (((0,), (0,)), ((), ()))
    v = v_ref[...]
    cell_dev = lax.dot_general(kw_h, v, dims, preferred_element_type=F32) + lax.dot_general(
        kw_l, v, dims, preferred_element_type=F32
    )

    def packed(cell, stab, tot):
        numbers = jnp.where(
            iota((8, HEAD_DIM), 0) == 0,
            jnp.broadcast_to(stab, (8, HEAD_DIM)),
            jnp.broadcast_to(tot, (8, HEAD_DIM)),
        )
        return jnp.concatenate([cell, numbers], axis=0)

    row_s[x] = packed(cell_dev, stab_dev, total)
    q = q_ref[...]
    scores = lax.dot_general(
        q, k_ref[...], (((1,), (1,)), ((), ())), preferred_element_type=F32
    ) * scale
    inner = jnp.where(causal, c_col - c_row + i_row, floor_neg)
    top = jnp.max(inner, axis=1, keepdims=True)
    p_h, p_l = two_parts(scores * jnp.exp(inner - top))
    num_s[...] = dot(p_h, v) + dot(p_l, v)

    def part_of(n, size):
        return jnp.floor((n.astype(F32) + 0.5) * (1.0 / size))

    same = part_of(iota((LEN, 1), 0), TOK) == part_of(iota((1, LEN), 1), TOK)
    earlier = jnp.where(same & (tt < ss), 1.0, 0.0).astype(BF16)
    named = [iota((NSP, LEN), 0) == route_ref[i : i + 1, :] for i in range(2)]
    onehot = [jnp.where(n, 1.0, 0.0) for n in named]
    ahead = dot((onehot[0] + onehot[1]).astype(BF16), earlier)
    places = [jnp.sum(ahead * o, axis=0, keepdims=True) for o in onehot]
    line = iota((HEAD_DIM, LEN), 0)
    rows = jnp.zeros((HEAD_DIM, LEN), F32)
    for i in range(2):
        rows = jnp.where(line == i, route_ref[i : i + 1, :].astype(F32) * SLOT + places[i], rows)
        rows = jnp.where(line == i + 2, weight_ref[i : i + 1, :], rows)
    table[...] = jnp.transpose(rows)

    def spots(tokens):
        return [
            jnp.concatenate([tokens[:, i : i + 1] + CAP * j for j in range(GT)], axis=0)
            for i in range(2)
        ]

    def block_rows(block):
        return pl.ds(pl.multiple_of(block * TOK, 8), TOK)

    place = iota((HROWS, ROWS), 1).astype(F32)
    for target, block in ((pick, tp), (pick_next, after)):
        first, second = spots(table[block_rows(block), :])
        target[...] = jnp.transpose(
            jnp.where((place == first) | (place == second), 1.0, 0.0)
        ).astype(BF16)

    def reordered(outer, middle):
        n = iota((ROWS, 1), 0)
        a = part_of(n, outer)
        rest = n.astype(F32) - outer * a
        b = jnp.floor((rest + 0.5) * (1.0 / CAP))
        source = b * middle + a * CAP + (rest - CAP * b)
        return jnp.where(iota((ROWS, ROWS), 1).astype(F32) == source, 1.0, 0.0).astype(BF16)

    pin[...] = reordered(PER, SLOT)
    pout[...] = reordered(SLOT, PER)

    pl.semaphore_wait(barrier, NSP - 1 + 3)

    def row_copy_x(i):
        return pltpu.make_async_remote_copy(
            src_ref=row_s.at[x], dst_ref=row_s.at[x], send_sem=row_ss.at[i], recv_sem=row_rs.at[x],
            device_id={"sp": y * NX + lax.rem(x + i, NX), "tp": tp}, device_id_type=MESH,
        )

    def row_arrival(source):
        return pltpu.make_async_remote_copy(
            src_ref=row_s.at[source], dst_ref=row_s.at[source],
            send_sem=row_ss.at[0], recv_sem=row_rs.at[source],
            device_id={"sp": sp, "tp": mate}, device_id_type=MESH,
        )

    def total_row_copy(to, source):
        return pltpu.make_async_remote_copy(
            src_ref=tot_send, dst_ref=tot_s.at[source],
            send_sem=tot_ss.at[to], recv_sem=tot_rs.at[source],
            device_id={"sp": to * NX + x, "tp": tp}, device_id_type=MESH,
        )

    for i in range(1, NX):
        row_copy_x(i).start()

    pairs = [(wo_hbm, wv.at[1]), (gate_hbm, gw.at[2]), (up_hbm, gw.at[3]), (down_hbm, dn.at[1])]
    shared = [
        pltpu.make_async_remote_copy(
            src_ref=source, dst_ref=target, send_sem=wx_send.at[i], recv_sem=wx_recv.at[i],
            device_id={"sp": sp, "tp": mate}, device_id_type=MESH,
        )
        for i, (source, target) in enumerate(pairs)
    ]
    for copy in shared:
        copy.start()

    for i in range(1, NX):
        row_arrival(lax.rem(x + i, NX)).wait_recv()

    low = jnp.full((1, HEAD_DIM), floor_neg, F32)
    none = jnp.zeros((1, HEAD_DIM), F32)
    blank = jnp.zeros((HEAD_DIM, HEAD_DIM), F32)

    def fold(buffer, at, count, carry):
        def one(i, carry):
            top, tot = carry
            n = count - 1 - i
            here = buffer[n, HEAD_DIM : HEAD_DIM + 1, :] + tot
            gs[at + n, 0:1, :] = here
            return jnp.maximum(top, here), tot + buffer[n, HEAD_DIM + 1 : HEAD_DIM + 2, :]

        return lax.fori_loop(0, count, one, carry)

    def weighted(buffer, at, count, stab, cell):
        def one(n, cell):
            return cell + jnp.exp(gs[at + n, 0:1, :] - stab) * buffer[n, :HEAD_DIM, :]

        return lax.fori_loop(0, count, one, cell)

    row_stab, row_tot = fold(row_s, 0, NX, (low, none))
    tot_send[...] = packed(weighted(row_s, 0, NX, row_stab, blank), row_stab, row_tot)

    @pl.loop(y + 1, NX)
    def _(to):
        total_row_copy(to, y).start()

    carry = fold(row_s, 0, x, (low, none))

    @pl.loop(0, y)
    def _(source):
        total_row_copy(source, source).wait_recv()

    stab0, tot0 = fold(tot_s, NX, y, carry)
    start_stab = jnp.maximum(stab0, tot0)
    start_cell = weighted(row_s, 0, x, start_stab, blank)
    cell_h, cell_l = two_parts(weighted(tot_s, NX, y, start_stab, start_cell))
    carried = c_col + start_stab[:, 0:1]
    stab = jnp.maximum(top, carried)
    numer = jnp.exp(top - stab) * num_s[...] + jnp.exp(carried - stab) * (
        dot(q, cell_h) + dot(q, cell_l)
    )
    scaled = (
        numer
        * lax.rsqrt(jnp.mean(numer * numer, axis=1, keepdims=True) + norm_eps)
        * hg_ref[...]
    )
    co_f[...] = scaled / (1.0 + jnp.exp(-og_ref[...].astype(F32)))
    for i in range(NZ):
        mine = pl.multiple_of((2 * i + core) * TOK, 8)
        theirs = pl.multiple_of((2 * i + 1 - core) * TOK, 8)
        co_a[i * TOK : (i + 1) * TOK, :] = co_f[pl.ds(mine, TOK), :]
        co_b[i * TOK : (i + 1) * TOK, :] = co_f[pl.ds(theirs, TOK), :]
    co_send[...] = co_b[...].astype(BF16)
    swap = pltpu.make_async_remote_copy(
        src_ref=co_send, dst_ref=co_recv, send_sem=co_sem.at[0], recv_sem=co_sem.at[1],
        device_id={"sp": sp, "tp": mate}, device_id_type=MESH,
    )
    swap.start()
    mine_b = co_a[...].astype(BF16)

    for i in range(1, NX):
        row_copy_x(i).wait_send()

    @pl.loop(y + 1, NX)
    def _(to):
        total_row_copy(to, y).wait_send()

    loads[0].wait()
    shared[0].wait()
    swap.wait()
    both = jnp.concatenate([mine_b, co_recv[...]], axis=1)

    def project(h):
        @pl.loop(h * GT, (h + 1) * GT)
        def _(j):
            at = pl.ds(pl.multiple_of(j * WIDE, WIDE), WIDE)
            part = dot(both, wv[:, :, at].reshape(2 * HEAD_DIM, WIDE))
            for i in range(NZ):
                pf[i, pl.ds(pl.multiple_of(j * TOK, 8), TOK), :] = part[i * TOK : (i + 1) * TOK]

    srows = TROWS // STRIPES

    def hops(d, p):
        return 4 if (p % 2 == 0) == (d == 0) else 3

    def sum_copy(d, m, p):
        rows = pl.ds(p * srows, srows)
        return pltpu.make_async_remote_copy(
            src_ref=r1_send.at[d, m, rows], dst_ref=r1_recv.at[d, m, rows],
            send_sem=r1_ss.at[d, m, p], recv_sem=r1_rs.at[d, m, p],
            device_id={"sp": sp, "tp": (above, below)[d]}, device_id_type=MESH,
        )

    def sum_steps(h, m):
        for d in range(2):
            for p in sorted((2 * h, 2 * h + 1), key=lambda p: -hops(d, p)):
                left = hops(d, p) - m
                if left > 0:
                    rows = slice(p * srows, (p + 1) * srows)
                    part = pf[lax.rem(z + (left if d == 0 else NZ - left), NZ), rows]
                    if m > 0:
                        sum_copy(d, m - 1, p).wait_recv()
                        part = part + r1_recv[d, m - 1, rows].astype(F32)
                    r1_send[d, m, rows] = part.astype(BF16)
                    sum_copy(d, m, p).start()

    def slot_rows(s):
        return pl.ds(pl.multiple_of(s * SLOT, SLOT), SLOT)

    def to_experts(n, chosen, tokens):
        d_send[n] = dot(chosen[...], tokens).astype(BF16)

        @pl.loop(1, NSP)
        def _(i):
            to = lax.rem(sp + i, NSP)
            pltpu.make_async_remote_copy(
                src_ref=d_send.at[n, slot_rows(to)], dst_ref=d_recv.at[n, slot_rows(sp)],
                send_sem=d_ss.at[n], recv_sem=d_rs.at[n],
                device_id={"sp": to, "tp": tp}, device_id_type=MESH,
            ).start()

        d_recv[n, slot_rows(sp)] = d_send[n, slot_rows(sp)]

    next_copy = pltpu.make_async_remote_copy(
        src_ref=am.at[pl.ds(0, HROWS)], dst_ref=am_next,
        send_sem=a_sem.at[0], recv_sem=a_sem.at[1],
        device_id={"sp": sp, "tp": before}, device_id_type=MESH,
    )

    def dispatch(h):
        for p in (2 * h, 2 * h + 1):
            rows = slice(p * srows, (p + 1) * srows)
            for d in range(2):
                sum_copy(d, hops(d, p) - 1, p).wait_recv()
            sides = [r1_recv[d, hops(d, p) - 1, rows].astype(F32) for d in range(2)]
            width = srows // TOK
            old = jnp.concatenate(
                [
                    resid[:, j * WIDE : (j + 1) * WIDE].astype(F32)
                    for j in range(p * width, (p + 1) * width)
                ],
                axis=0,
            )
            am[rows] = (old + (pf[z, rows] + sides[0] + sides[1])).astype(BF16)
        if h == 0:
            next_copy.start()
        to_experts(h, pick, am[h * HROWS : (h + 1) * HROWS])

    project(0)
    sum_steps(0, 0)
    project(1)
    loads[4].wait()
    for m in range(1, 4):
        sum_steps(0, m)
        sum_steps(1, m - 1)
    dispatch(0)
    sum_steps(1, 3)
    dispatch(1)

    next_copy.wait_recv()
    to_experts(TURNS, pick_next, am_next[...])

    for load in loads[1:4]:
        load.wait()
    for copy in shared[1:]:
        copy.wait()

    others = pl.ds(0, ROWS - SLOT)
    xrows = ROWS // PIECES

    def block_of(k):
        return lax.rem(z + NZ * NZ - step * k, NZ)

    def row_copy(k, h, p):
        rows = pl.ds(pl.multiple_of(p * xrows, xrows), xrows)
        return pltpu.make_async_remote_copy(
            src_ref=xring.at[k, h, rows], dst_ref=xring.at[k + 1, h, rows],
            send_sem=x_ss.at[k, h, p], recv_sem=x_rs.at[k, h, p],
            device_id={"sp": sp, "tp": after}, device_id_type=MESH,
        )

    def total_copy(k, h):
        return pltpu.make_async_remote_copy(
            src_ref=r2_send.at[k, h], dst_ref=r2_recv.at[k + 1, h],
            send_sem=r2_ss.at[k, h], recv_sem=r2_rs.at[k + 1, h],
            device_id={"sp": sp, "tp": after}, device_id_type=MESH,
        )

    def from_plane(k, h, n):
        pltpu.make_async_copy(d_recv.at[n, others], d_recv.at[n, others], d_rs.at[n]).wait()
        xring[k, h] = dot(pin[...], d_recv[n]).astype(BF16)

    def arrive(k, h):
        @pl.when(k == 0)
        def _():
            from_plane(0, h, h)

        last = NZ - 2 if h == 0 else NZ - 1

        @pl.loop(0, PIECES)
        def _(p):
            @pl.when((k > 0) & (k <= last))
            def _():
                row_copy(k - 1, h, p).wait_recv()

            @pl.when(k < last)
            def _():
                row_copy(k, h, p).start()

        if h == 0:
            @pl.when(k == NZ - 1)
            def _():
                from_plane(NZ - 1, h, TURNS)

    def first_part(k, h):
        acc = jnp.zeros((PER, 4 * HEAD_DIM), F32)
        squares = jnp.zeros((PER, WIDE), F32)
        for j in range(GT):
            at = slice((h * GT + j) * WIDE, (h * GT + j + 1) * WIDE)
            rows = xring[k, h, j * PER : (j + 1) * PER, :].astype(F32)
            squares = squares + rows * rows
            w = jnp.concatenate([gw[i, at, :] for i in range(4)], axis=1)
            acc = acc + dot((rows * eng_ref[:, at]).astype(BF16), w)
        return acc, squares

    def second_part(k, acc, squares):
        mean = jnp.sum(squares, axis=1, keepdims=True) * (1.0 / (GROUPS * WIDE))
        acc = acc * lax.rsqrt(mean + norm_eps)
        acts = []
        for i in range(2):
            gate = acc[:, 2 * i * HEAD_DIM : (2 * i + 1) * HEAD_DIM]
            upper = acc[:, (2 * i + 1) * HEAD_DIM : (2 * i + 2) * HEAD_DIM]
            acts.append((gate / (1.0 + jnp.exp(-gate)) * upper).astype(BF16))
        act = jnp.concatenate(acts, axis=1)
        for h in range(TURNS):
            for j in range(GT):
                at = slice((h * GT + j) * WIDE, (h * GT + j + 1) * WIDE)
                w = dn[:, :, at].reshape(2 * HEAD_DIM, WIDE)
                ybuf[h, j * PER : (j + 1) * PER, :] = dot(act, w).astype(BF16)
            t_send[k, h] = dot(pout[...], ybuf[h]).astype(BF16)

            @pl.loop(1, NSP)
            def _(i, h=h):
                to = lax.rem(sp + i, NSP)
                pltpu.make_async_remote_copy(
                    src_ref=t_send.at[k, h, slot_rows(to)], dst_ref=t_recv.at[k, h, slot_rows(sp)],
                    send_sem=t_ss.at[k, h], recv_sem=t_rs.at[k, h],
                    device_id={"sp": to, "tp": tp}, device_id_type=MESH,
                ).start()

            t_recv[k, h, slot_rows(sp)] = t_send[k, h, slot_rows(sp)]

    def combine(k, h):
        if h == 0:
            tokens = table[block_rows(block_of(k) * 2 + core), :]
            first, second = spots(tokens)
            weights = [jnp.concatenate([tokens[:, i : i + 1]] * GT, axis=0) for i in (2, 3)]
            place = iota((HROWS, ROWS), 1).astype(F32)
            weight = jnp.where(place == first, weights[0], 0.0) + jnp.where(
                place == second, weights[1], 0.0
            )
            w_h, w_l = two_parts(weight)
            mixer[:HROWS] = w_h
            mixer[HROWS:] = w_l
        pltpu.make_async_copy(
            t_recv.at[k, h, others], t_recv.at[k, h, others], t_rs.at[k, h]
        ).wait()
        mixed = dot(mixer[...], t_recv[k, h])
        mixed = mixed[:HROWS] + mixed[HROWS:]

        @pl.when(k == 0)
        def _():
            own[h] = mixed

        @pl.when(k == 1)
        def _():
            r2_send[k, h] = mixed.astype(BF16)
            total_copy(k, h).start()

        @pl.when(k > 1)
        def _():
            total_copy(k - 1, h).wait_recv()
            r2_send[k, h] = (mixed + r2_recv[k, h].astype(F32)).astype(BF16)
            total_copy(k, h).start()

    @pl.loop(0, NZ)
    def _(k):
        arrive(k, 0)
        acc, squares = first_part(k, 0)
        acc_s[...] = acc
        sq_s[...] = squares

        @pl.when(k >= LAG)
        def _():
            combine(k - LAG, 0)

        arrive(k, 1)
        acc, squares = first_part(k, 1)
        second_part(k, acc_s[...] + acc, sq_s[...] + squares)

        @pl.when(k >= LAG)
        def _():
            combine(k - LAG, 1)

    @pl.loop(NZ - LAG, NZ)
    def _(k):
        for h in range(TURNS):
            combine(k, h)

    for h in range(TURNS):
        total_copy(NZ - 1, h).wait_recv()
        result = am[h * HROWS : (h + 1) * HROWS].astype(F32) + (
            own[h] + r2_recv[NZ, h].astype(F32)
        )
        for j in range(GT):
            at = slice((h * GT + j) * WIDE, (h * GT + j + 1) * WIDE)
            out_ref[:, at] = result[j * TOK : (j + 1) * TOK].astype(BF16)

    for d in range(2):
        for p in range(STRIPES):
            for m in range(hops(d, p)):
                sum_copy(d, m, p).wait_send()

    @pl.loop(1, NZ)
    def _(k):
        @pl.loop(0, TURNS)
        def _(h):
            total_copy(k, h).wait_send()

            @pl.when((h > 0) | (k < NZ - 1))
            def _():
                @pl.loop(0, PIECES)
                def _(p):
                    row_copy(k - 1, h, p).wait_send()

    next_copy.wait_send()

    @pl.loop(0, TURNS + 1)
    def _(n):
        pltpu.make_async_copy(d_send.at[n, others], d_send.at[n, others], d_ss.at[n]).wait()

    @pl.loop(0, TURNS)
    def _(h):
        @pl.loop(0, NZ)
        def _(k):
            pltpu.make_async_copy(
                t_send.at[k, h, others], t_send.at[k, h, others], t_ss.at[k, h]
            ).wait()


def local(
    queries,
    cell_key_rows,
    cell_value_rows,
    output_gate_logits,
    input_gate_logs,
    forget_gate_logits,
    extra_log_forget,
    head_norm_gain,
    cell_output_matrix,
    residual,
    expert_norm_gain,
    routes,
    token_expert_weights,
    expert_gate_matrix,
    expert_up_matrix,
    expert_down_matrix,
):
    vmem = pl.BlockSpec(memory_space=pltpu.VMEM)
    hbm = pl.BlockSpec(memory_space=pltpu.HBM)
    dma = pltpu.SemaphoreType.DMA
    width = GROUPS * WIDE
    return pl.pallas_call(
        kernel,
        name="layer",
        out_shape=jax.ShapeDtypeStruct((TOK, width), BF16),
        in_specs=[vmem] * 11 + [hbm] * 5,
        out_specs=vmem,
        scratch_shapes=[
            pltpu.VMEM((2, HEAD_DIM, width), BF16),
            pltpu.VMEM((4, width, HEAD_DIM), BF16),
            pltpu.VMEM((2, HEAD_DIM, width), BF16),
            pltpu.VMEM((TOK, width), BF16),
            pltpu.VMEM((NX, HEAD_DIM + 8, HEAD_DIM), F32),
            pltpu.VMEM((HEAD_DIM + 8, HEAD_DIM), F32),
            pltpu.VMEM((NX, HEAD_DIM + 8, HEAD_DIM), F32),
            pltpu.VMEM((NSP, 8, HEAD_DIM), F32),
            pltpu.VMEM((LEN, HEAD_DIM), F32),
            pltpu.VMEM((LEN, HEAD_DIM), F32),
            pltpu.VMEM((LEN // 2, HEAD_DIM), F32),
            pltpu.VMEM((LEN // 2, HEAD_DIM), F32),
            pltpu.VMEM((LEN // 2, HEAD_DIM), BF16),
            pltpu.VMEM((LEN // 2, HEAD_DIM), BF16),
            pltpu.VMEM((NZ, TROWS, WIDE), F32),
            pltpu.VMEM((2, 4, TROWS, WIDE), BF16),
            pltpu.VMEM((2, 4, TROWS, WIDE), BF16),
            pltpu.VMEM((TROWS, WIDE), BF16),
            pltpu.VMEM((TURNS + 1, ROWS, WIDE), BF16),
            pltpu.VMEM((TURNS + 1, ROWS, WIDE), BF16),
            pltpu.VMEM((HROWS, WIDE), BF16),
            pltpu.VMEM((ROWS, ROWS), BF16),
            pltpu.VMEM((ROWS, ROWS), BF16),
            pltpu.VMEM((ROWS, HROWS), BF16),
            pltpu.VMEM((ROWS, HROWS), BF16),
            pltpu.VMEM((LEN, HEAD_DIM), F32),
            pltpu.VMEM((NZ, TURNS, ROWS, WIDE), BF16),
            pltpu.VMEM((PER, 4 * HEAD_DIM), F32),
            pltpu.VMEM((PER, WIDE), F32),
            pltpu.VMEM((TURNS, ROWS, WIDE), BF16),
            pltpu.VMEM((2 * HROWS, ROWS), BF16),
            pltpu.VMEM((NZ, TURNS, ROWS, WIDE), BF16),
            pltpu.VMEM((NZ, TURNS, ROWS, WIDE), BF16),
            pltpu.VMEM((NZ, TURNS, HROWS, WIDE), BF16),
            pltpu.VMEM((NZ + 1, TURNS, HROWS, WIDE), BF16),
            pltpu.VMEM((TURNS, HROWS, WIDE), F32),
            dma((5,)), dma((4,)), dma((4,)), dma((NX,)), dma((NX,)), dma((NX,)), dma((NX,)), dma((2,)),
            dma((2, 4, STRIPES)), dma((2, 4, STRIPES)),
            dma((TURNS + 1,)), dma((TURNS + 1,)), dma((2,)),
            dma((NZ - 1, TURNS, PIECES)), dma((NZ - 1, TURNS, PIECES)),
            dma((NZ, TURNS)), dma((NZ, TURNS)), dma((NZ, TURNS)), dma((NZ + 1, TURNS)),
        ],
        compiler_params=pltpu.CompilerParams(
            collective_id=0, has_side_effects=True, vmem_limit_bytes=60 << 20
        ),
    )(
        queries,
        cell_key_rows,
        cell_value_rows,
        output_gate_logits,
        input_gate_logs,
        forget_gate_logits,
        extra_log_forget,
        head_norm_gain.reshape(1, HEAD_DIM),
        expert_norm_gain.reshape(1, width),
        routes.T,
        token_expert_weights.T,
        residual,
        cell_output_matrix,
        expert_gate_matrix[0],
        expert_up_matrix[0],
        expert_down_matrix[0],
    )


def solution(mesh):
    in_specs = (
        P("sp", "tp"),
        P("sp", "tp"),
        P("sp", "tp"),
        P("sp", "tp"),
        P("tp", "sp"),
        P("tp", "sp"),
        P("tp", "sp"),
        P("tp"),
        P("tp", None),
        P("sp", None),
        P(),
        P("sp", None),
        P("sp", None),
        P("sp", None, "tp"),
        P("sp", None, "tp"),
        P("sp", "tp", None),
    )
    return jax.shard_map(
        local, mesh=mesh, in_specs=in_specs, out_specs=P(("sp", "tp"), None), check_vma=False
    )
```

```python
import jax
import jax.numpy as jnp
from jax import lax
from jax.experimental import pallas as pl
from jax.experimental.pallas import tpu as pltpu
from jax.sharding import PartitionSpec as P

MESH = pl.DeviceIdType.MESH
F32 = jnp.float32
BF16 = jnp.bfloat16

HEAD_DIM = 128
NSP = 16
NZ = 8
LEN = 384
TOK = 24
CAP = 6
GROUPS = 16
WIDE = 256
TURNS = 2
GT = GROUPS // TURNS
SLOT = GT * CAP
ROWS = NSP * SLOT
TROWS = GROUPS * TOK
HROWS = GT * TOK
PER = ROWS // GT
NX = 4
LAG = 2
PIECES = 2
STRIPES = 4

floor_neg = -1e30
norm_eps = 1e-06


def dot(a, b):
    return jnp.dot(a, b, preferred_element_type=F32)


def two_parts(x):
    high = x.astype(BF16)
    return high, (x - high.astype(F32)).astype(BF16)


def iota(shape, dim):
    return lax.broadcasted_iota(jnp.int32, shape, dim)


def kernel(
    q_ref, k_ref, v_ref, og_ref, ig_ref, fg_ref, ex_ref, hg_ref,
    eng_ref, route_ref, weight_ref,
    resid_hbm, wo_hbm, gate_hbm, up_hbm, down_hbm,
    out_ref,
    wv, gw, dn, resid,
    row_s, tot_send, tot_s, gs, num_s, co_f, co_a, co_b, co_send, co_recv,
    pf, r1_send, r1_recv, am,
    d_send, d_recv, am_next, pin, pout, pick, pick_next, table,
    xring, acc_s, sq_s, ybuf, mixer, t_send, t_recv, r2_send, r2_recv, own,
    load_sem, wx_send, wx_recv, row_ss, row_rs, tot_ss, tot_rs, co_sem, r1_ss, r1_rs,
    d_ss, d_rs, a_sem, x_ss, x_rs, t_ss, t_rs, r2_ss, r2_rs,
):
    sp = lax.axis_index("sp")
    tp = lax.axis_index("tp")
    core = lax.rem(tp, 2)
    z = tp // 2
    step = jnp.where(core == 0, 1, NZ - 1)
    above = lax.rem(z + 1, NZ) * 2 + core
    below = lax.rem(z + NZ - 1, NZ) * 2 + core
    after = jnp.where(core == 0, above, below)
    before = jnp.where(core == 0, below, above)
    mate = z * 2 + 1 - core
    y, x = sp // NX, lax.rem(sp, NX)

    barrier = pltpu.get_barrier_semaphore()

    @pl.loop(1, NSP)
    def _(i):
        pl.semaphore_signal(
            barrier, inc=1, device_id={"sp": lax.rem(sp + i, NSP), "tp": tp}, device_id_type=MESH
        )

    for other in (above, below, mate):
        pl.semaphore_signal(barrier, inc=1, device_id={"sp": sp, "tp": other}, device_id_type=MESH)

    loads = [
        pltpu.make_async_copy(wo_hbm, wv.at[0], load_sem.at[0]),
        pltpu.make_async_copy(gate_hbm, gw.at[0], load_sem.at[1]),
        pltpu.make_async_copy(up_hbm, gw.at[1], load_sem.at[2]),
        pltpu.make_async_copy(down_hbm, dn.at[0], load_sem.at[3]),
        pltpu.make_async_copy(
            resid_hbm.at[pl.ds(pl.multiple_of(tp * TOK, 8), TOK)], resid, load_sem.at[4]
        ),
    ]
    for load in loads:
        load.start()

    tt = iota((LEN, LEN), 0)
    ss = iota((LEN, LEN), 1)
    causal = ss <= tt
    fg = fg_ref[...]
    f_row = jnp.minimum(fg, 0.0) - jnp.log1p(jnp.exp(-jnp.abs(fg))) + ex_ref[...]
    i_row = ig_ref[...]
    f_all = jnp.broadcast_to(f_row, (LEN, LEN))
    f_col = jnp.sum(jnp.where(ss == tt, f_all, 0.0), axis=1, keepdims=True)
    i_col = jnp.sum(
        jnp.where(ss == tt, jnp.broadcast_to(i_row, (LEN, LEN)), 0.0), axis=1, keepdims=True
    )
    c_col = jnp.sum(jnp.where(causal, f_all, 0.0), axis=1, keepdims=True)
    c_row = jnp.sum(
        jnp.where(tt <= ss, jnp.broadcast_to(f_col, (LEN, LEN)), 0.0), axis=0, keepdims=True
    )
    total = jnp.sum(f_row, axis=1, keepdims=True)
    scale = HEAD_DIM ** (-0.5)
    write = i_col + total - c_col
    stab_dev = jnp.max(write, axis=0, keepdims=True)
    kw = k_ref[...].astype(F32) * (jnp.exp(write - stab_dev) * scale)
    kw_h, kw_l = two_parts(kw)
    dims = (((0,), (0,)), ((), ()))
    v = v_ref[...]
    cell_dev = lax.dot_general(kw_h, v, dims, preferred_element_type=F32) + lax.dot_general(
        kw_l, v, dims, preferred_element_type=F32
    )

    def packed(cell, stab, tot):
        numbers = jnp.where(
            iota((8, HEAD_DIM), 0) == 0,
            jnp.broadcast_to(stab, (8, HEAD_DIM)),
            jnp.broadcast_to(tot, (8, HEAD_DIM)),
        )
        return jnp.concatenate([cell, numbers], axis=0)

    row_s[x] = packed(cell_dev, stab_dev, total)
    q = q_ref[...]
    scores = lax.dot_general(
        q, k_ref[...], (((1,), (1,)), ((), ())), preferred_element_type=F32
    ) * scale
    inner = jnp.where(causal, c_col - c_row + i_row, floor_neg)
    top = jnp.max(inner, axis=1, keepdims=True)
    p_h, p_l = two_parts(scores * jnp.exp(inner - top))
    num_s[...] = dot(p_h, v) + dot(p_l, v)

    def part_of(n, size):
        return jnp.floor((n.astype(F32) + 0.5) * (1.0 / size))

    same = part_of(iota((LEN, 1), 0), TOK) == part_of(iota((1, LEN), 1), TOK)
    earlier = jnp.where(same & (tt < ss), 1.0, 0.0).astype(BF16)
    named = [iota((NSP, LEN), 0) == route_ref[i : i + 1, :] for i in range(2)]
    onehot = [jnp.where(n, 1.0, 0.0) for n in named]
    ahead = dot((onehot[0] + onehot[1]).astype(BF16), earlier)
    places = [jnp.sum(ahead * o, axis=0, keepdims=True) for o in onehot]
    line = iota((HEAD_DIM, LEN), 0)
    rows = jnp.zeros((HEAD_DIM, LEN), F32)
    for i in range(2):
        rows = jnp.where(line == i, route_ref[i : i + 1, :].astype(F32) * SLOT + places[i], rows)
        rows = jnp.where(line == i + 2, weight_ref[i : i + 1, :], rows)
    table[...] = jnp.transpose(rows)

    def spots(tokens):
        return [
            jnp.concatenate([tokens[:, i : i + 1] + CAP * j for j in range(GT)], axis=0)
            for i in range(2)
        ]

    def block_rows(block):
        return pl.ds(pl.multiple_of(block * TOK, 8), TOK)

    place = iota((HROWS, ROWS), 1).astype(F32)
    for target, block in ((pick, tp), (pick_next, after)):
        first, second = spots(table[block_rows(block), :])
        target[...] = jnp.transpose(
            jnp.where((place == first) | (place == second), 1.0, 0.0)
        ).astype(BF16)

    def reordered(outer, middle):
        n = iota((ROWS, 1), 0)
        a = part_of(n, outer)
        rest = n.astype(F32) - outer * a
        b = jnp.floor((rest + 0.5) * (1.0 / CAP))
        source = b * middle + a * CAP + (rest - CAP * b)
        return jnp.where(iota((ROWS, ROWS), 1).astype(F32) == source, 1.0, 0.0).astype(BF16)

    pin[...] = reordered(PER, SLOT)
    pout[...] = reordered(SLOT, PER)

    pl.semaphore_wait(barrier, NSP - 1 + 3)

    def row_copy_x(i):
        return pltpu.make_async_remote_copy(
            src_ref=row_s.at[x], dst_ref=row_s.at[x], send_sem=row_ss.at[i], recv_sem=row_rs.at[x],
            device_id={"sp": y * NX + lax.rem(x + i, NX), "tp": tp}, device_id_type=MESH,
        )

    def row_arrival(source):
        return pltpu.make_async_remote_copy(
            src_ref=row_s.at[source], dst_ref=row_s.at[source],
            send_sem=row_ss.at[0], recv_sem=row_rs.at[source],
            device_id={"sp": sp, "tp": mate}, device_id_type=MESH,
        )

    def total_row_copy(to, source):
        return pltpu.make_async_remote_copy(
            src_ref=tot_send, dst_ref=tot_s.at[source],
            send_sem=tot_ss.at[to], recv_sem=tot_rs.at[source],
            device_id={"sp": to * NX + x, "tp": tp}, device_id_type=MESH,
        )

    for i in range(1, NX):
        row_copy_x(i).start()

    pairs = [(wo_hbm, wv.at[1]), (gate_hbm, gw.at[2]), (up_hbm, gw.at[3]), (down_hbm, dn.at[1])]
    shared = [
        pltpu.make_async_remote_copy(
            src_ref=source, dst_ref=target, send_sem=wx_send.at[i], recv_sem=wx_recv.at[i],
            device_id={"sp": sp, "tp": mate}, device_id_type=MESH,
        )
        for i, (source, target) in enumerate(pairs)
    ]
    for copy in shared:
        copy.start()

    for i in range(1, NX):
        row_arrival(lax.rem(x + i, NX)).wait_recv()

    low = jnp.full((1, HEAD_DIM), floor_neg, F32)
    none = jnp.zeros((1, HEAD_DIM), F32)
    blank = jnp.zeros((HEAD_DIM, HEAD_DIM), F32)

    def fold(buffer, at, count, carry):
        def one(i, carry):
            top, tot = carry
            n = count - 1 - i
            here = buffer[n, HEAD_DIM : HEAD_DIM + 1, :] + tot
            gs[at + n, 0:1, :] = here
            return jnp.maximum(top, here), tot + buffer[n, HEAD_DIM + 1 : HEAD_DIM + 2, :]

        return lax.fori_loop(0, count, one, carry)

    def weighted(buffer, at, count, stab, cell):
        def one(n, cell):
            return cell + jnp.exp(gs[at + n, 0:1, :] - stab) * buffer[n, :HEAD_DIM, :]

        return lax.fori_loop(0, count, one, cell)

    row_stab, row_tot = fold(row_s, 0, NX, (low, none))
    tot_send[...] = packed(weighted(row_s, 0, NX, row_stab, blank), row_stab, row_tot)

    @pl.loop(y + 1, NX)
    def _(to):
        total_row_copy(to, y).start()

    carry = fold(row_s, 0, x, (low, none))

    @pl.loop(0, y)
    def _(source):
        total_row_copy(source, source).wait_recv()

    stab0, tot0 = fold(tot_s, NX, y, carry)
    start_stab = jnp.maximum(stab0, tot0)
    start_cell = weighted(row_s, 0, x, start_stab, blank)
    cell_h, cell_l = two_parts(weighted(tot_s, NX, y, start_stab, start_cell))
    carried = c_col + start_stab[:, 0:1]
    stab = jnp.maximum(top, carried)
    numer = jnp.exp(top - stab) * num_s[...] + jnp.exp(carried - stab) * (
        dot(q, cell_h) + dot(q, cell_l)
    )
    scaled = (
        numer
        * lax.rsqrt(jnp.mean(numer * numer, axis=1, keepdims=True) + norm_eps)
        * hg_ref[...]
    )
    co_f[...] = scaled / (1.0 + jnp.exp(-og_ref[...].astype(F32)))
    for i in range(NZ):
        mine = pl.multiple_of((2 * i + core) * TOK, 8)
        theirs = pl.multiple_of((2 * i + 1 - core) * TOK, 8)
        co_a[i * TOK : (i + 1) * TOK, :] = co_f[pl.ds(mine, TOK), :]
        co_b[i * TOK : (i + 1) * TOK, :] = co_f[pl.ds(theirs, TOK), :]
    co_send[...] = co_b[...].astype(BF16)
    swap = pltpu.make_async_remote_copy(
        src_ref=co_send, dst_ref=co_recv, send_sem=co_sem.at[0], recv_sem=co_sem.at[1],
        device_id={"sp": sp, "tp": mate}, device_id_type=MESH,
    )
    swap.start()
    mine_b = co_a[...].astype(BF16)

    for i in range(1, NX):
        row_copy_x(i).wait_send()

    @pl.loop(y + 1, NX)
    def _(to):
        total_row_copy(to, y).wait_send()

    loads[0].wait()
    shared[0].wait()
    swap.wait()
    both = jnp.concatenate([mine_b, co_recv[...]], axis=1)

    def project(h):
        @pl.loop(h * GT, (h + 1) * GT)
        def _(j):
            at = pl.ds(pl.multiple_of(j * WIDE, WIDE), WIDE)
            part = dot(both, wv[:, :, at].reshape(2 * HEAD_DIM, WIDE))
            for i in range(NZ):
                pf[i, pl.ds(pl.multiple_of(j * TOK, 8), TOK), :] = part[i * TOK : (i + 1) * TOK]

    srows = TROWS // STRIPES

    def hops(d, p):
        return 4 if (p % 2 == 0) == (d == 0) else 3

    def sum_copy(d, m, p):
        rows = pl.ds(p * srows, srows)
        return pltpu.make_async_remote_copy(
            src_ref=r1_send.at[d, m, rows], dst_ref=r1_recv.at[d, m, rows],
            send_sem=r1_ss.at[d, m, p], recv_sem=r1_rs.at[d, m, p],
            device_id={"sp": sp, "tp": (above, below)[d]}, device_id_type=MESH,
        )

    def sum_steps(h, m):
        for d in range(2):
            for p in sorted((2 * h, 2 * h + 1), key=lambda p: -hops(d, p)):
                left = hops(d, p) - m
                if left > 0:
                    rows = slice(p * srows, (p + 1) * srows)
                    part = pf[lax.rem(z + (left if d == 0 else NZ - left), NZ), rows]
                    if m > 0:
                        sum_copy(d, m - 1, p).wait_recv()
                        part = part + r1_recv[d, m - 1, rows].astype(F32)
                    r1_send[d, m, rows] = part.astype(BF16)
                    sum_copy(d, m, p).start()

    def slot_rows(s):
        return pl.ds(pl.multiple_of(s * SLOT, SLOT), SLOT)

    def to_experts(n, chosen, tokens):
        d_send[n] = dot(chosen[...], tokens).astype(BF16)

        @pl.loop(1, NSP)
        def _(i):
            to = lax.rem(sp + i, NSP)
            pltpu.make_async_remote_copy(
                src_ref=d_send.at[n, slot_rows(to)], dst_ref=d_recv.at[n, slot_rows(sp)],
                send_sem=d_ss.at[n], recv_sem=d_rs.at[n],
                device_id={"sp": to, "tp": tp}, device_id_type=MESH,
            ).start()

        d_recv[n, slot_rows(sp)] = d_send[n, slot_rows(sp)]

    next_copy = pltpu.make_async_remote_copy(
        src_ref=am.at[pl.ds(0, HROWS)], dst_ref=am_next,
        send_sem=a_sem.at[0], recv_sem=a_sem.at[1],
        device_id={"sp": sp, "tp": before}, device_id_type=MESH,
    )

    def dispatch(h):
        for p in (2 * h, 2 * h + 1):
            rows = slice(p * srows, (p + 1) * srows)
            for d in range(2):
                sum_copy(d, hops(d, p) - 1, p).wait_recv()
            sides = [r1_recv[d, hops(d, p) - 1, rows].astype(F32) for d in range(2)]
            width = srows // TOK
            old = jnp.concatenate(
                [
                    resid[:, j * WIDE : (j + 1) * WIDE].astype(F32)
                    for j in range(p * width, (p + 1) * width)
                ],
                axis=0,
            )
            am[rows] = (old + (pf[z, rows] + sides[0] + sides[1])).astype(BF16)
        if h == 0:
            next_copy.start()
        to_experts(h, pick, am[h * HROWS : (h + 1) * HROWS])

    project(0)
    sum_steps(0, 0)
    project(1)
    loads[4].wait()
    for m in range(1, 4):
        sum_steps(0, m)
        sum_steps(1, m - 1)
    dispatch(0)
    sum_steps(1, 3)
    dispatch(1)

    next_copy.wait_recv()
    to_experts(TURNS, pick_next, am_next[...])

    for load in loads[1:4]:
        load.wait()
    for copy in shared[1:]:
        copy.wait()

    others = pl.ds(0, ROWS - SLOT)
    xrows = ROWS // PIECES

    def block_of(k):
        return lax.rem(z + NZ * NZ - step * k, NZ)

    def row_copy(k, h, p):
        rows = pl.ds(pl.multiple_of(p * xrows, xrows), xrows)
        return pltpu.make_async_remote_copy(
            src_ref=xring.at[k, h, rows], dst_ref=xring.at[k + 1, h, rows],
            send_sem=x_ss.at[k, h, p], recv_sem=x_rs.at[k, h, p],
            device_id={"sp": sp, "tp": after}, device_id_type=MESH,
        )

    def total_copy(k, h):
        return pltpu.make_async_remote_copy(
            src_ref=r2_send.at[k, h], dst_ref=r2_recv.at[k + 1, h],
            send_sem=r2_ss.at[k, h], recv_sem=r2_rs.at[k + 1, h],
            device_id={"sp": sp, "tp": after}, device_id_type=MESH,
        )

    def from_plane(k, h, n):
        pltpu.make_async_copy(d_recv.at[n, others], d_recv.at[n, others], d_rs.at[n]).wait()
        xring[k, h] = dot(pin[...], d_recv[n]).astype(BF16)

    def arrive(k, h):
        @pl.when(k == 0)
        def _():
            from_plane(0, h, h)

        last = NZ - 2 if h == 0 else NZ - 1

        @pl.loop(0, PIECES)
        def _(p):
            @pl.when((k > 0) & (k <= last))
            def _():
                row_copy(k - 1, h, p).wait_recv()

            @pl.when(k < last)
            def _():
                row_copy(k, h, p).start()

        if h == 0:
            @pl.when(k == NZ - 1)
            def _():
                from_plane(NZ - 1, h, TURNS)

    def first_part(k, h):
        acc = jnp.zeros((PER, 4 * HEAD_DIM), F32)
        squares = jnp.zeros((PER, WIDE), F32)
        for j in range(GT):
            at = slice((h * GT + j) * WIDE, (h * GT + j + 1) * WIDE)
            rows = xring[k, h, j * PER : (j + 1) * PER, :].astype(F32)
            squares = squares + rows * rows
            w = jnp.concatenate([gw[i, at, :] for i in range(4)], axis=1)
            acc = acc + dot((rows * eng_ref[:, at]).astype(BF16), w)
        return acc, squares

    def second_part(k, acc, squares):
        mean = jnp.sum(squares, axis=1, keepdims=True) * (1.0 / (GROUPS * WIDE))
        acc = acc * lax.rsqrt(mean + norm_eps)
        acts = []
        for i in range(2):
            gate = acc[:, 2 * i * HEAD_DIM : (2 * i + 1) * HEAD_DIM]
            upper = acc[:, (2 * i + 1) * HEAD_DIM : (2 * i + 2) * HEAD_DIM]
            acts.append((gate / (1.0 + jnp.exp(-gate)) * upper).astype(BF16))
        act = jnp.concatenate(acts, axis=1)
        for h in range(TURNS):
            for j in range(GT):
                at = slice((h * GT + j) * WIDE, (h * GT + j + 1) * WIDE)
                w = dn[:, :, at].reshape(2 * HEAD_DIM, WIDE)
                ybuf[h, j * PER : (j + 1) * PER, :] = dot(act, w).astype(BF16)
            t_send[k, h] = dot(pout[...], ybuf[h]).astype(BF16)

            @pl.loop(1, NSP)
            def _(i, h=h):
                to = lax.rem(sp + i, NSP)
                pltpu.make_async_remote_copy(
                    src_ref=t_send.at[k, h, slot_rows(to)], dst_ref=t_recv.at[k, h, slot_rows(sp)],
                    send_sem=t_ss.at[k, h], recv_sem=t_rs.at[k, h],
                    device_id={"sp": to, "tp": tp}, device_id_type=MESH,
                ).start()

            t_recv[k, h, slot_rows(sp)] = t_send[k, h, slot_rows(sp)]

    def combine(k, h):
        if h == 0:
            tokens = table[block_rows(block_of(k) * 2 + core), :]
            first, second = spots(tokens)
            weights = [jnp.concatenate([tokens[:, i : i + 1]] * GT, axis=0) for i in (2, 3)]
            place = iota((HROWS, ROWS), 1).astype(F32)
            weight = jnp.where(place == first, weights[0], 0.0) + jnp.where(
                place == second, weights[1], 0.0
            )
            w_h, w_l = two_parts(weight)
            mixer[:HROWS] = w_h
            mixer[HROWS:] = w_l
        pltpu.make_async_copy(
            t_recv.at[k, h, others], t_recv.at[k, h, others], t_rs.at[k, h]
        ).wait()
        mixed = dot(mixer[...], t_recv[k, h])
        mixed = mixed[:HROWS] + mixed[HROWS:]

        @pl.when(k == 0)
        def _():
            own[h] = mixed

        @pl.when(k == 1)
        def _():
            r2_send[k, h] = mixed.astype(BF16)
            total_copy(k, h).start()

        @pl.when(k > 1)
        def _():
            total_copy(k - 1, h).wait_recv()
            r2_send[k, h] = (mixed + r2_recv[k, h].astype(F32)).astype(BF16)
            total_copy(k, h).start()

    @pl.loop(0, NZ)
    def _(k):
        arrive(k, 0)
        acc, squares = first_part(k, 0)
        acc_s[...] = acc
        sq_s[...] = squares

        arrive(k, 1)
        acc, squares = first_part(k, 1)
        second_part(k, acc_s[...] + acc, sq_s[...] + squares)

        @pl.when(k >= LAG)
        def _():
            combine(k - LAG, 0)
            combine(k - LAG, 1)

    @pl.loop(NZ - LAG, NZ)
    def _(k):
        for h in range(TURNS):
            combine(k, h)

    for h in range(TURNS):
        total_copy(NZ - 1, h).wait_recv()
        result = am[h * HROWS : (h + 1) * HROWS].astype(F32) + (
            own[h] + r2_recv[NZ, h].astype(F32)
        )
        for j in range(GT):
            at = slice((h * GT + j) * WIDE, (h * GT + j + 1) * WIDE)
            out_ref[:, at] = result[j * TOK : (j + 1) * TOK].astype(BF16)

    for d in range(2):
        for p in range(STRIPES):
            for m in range(hops(d, p)):
                sum_copy(d, m, p).wait_send()

    @pl.loop(1, NZ)
    def _(k):
        @pl.loop(0, TURNS)
        def _(h):
            total_copy(k, h).wait_send()

            @pl.when((h > 0) | (k < NZ - 1))
            def _():
                @pl.loop(0, PIECES)
                def _(p):
                    row_copy(k - 1, h, p).wait_send()

    next_copy.wait_send()

    @pl.loop(0, TURNS + 1)
    def _(n):
        pltpu.make_async_copy(d_send.at[n, others], d_send.at[n, others], d_ss.at[n]).wait()

    @pl.loop(0, TURNS)
    def _(h):
        @pl.loop(0, NZ)
        def _(k):
            pltpu.make_async_copy(
                t_send.at[k, h, others], t_send.at[k, h, others], t_ss.at[k, h]
            ).wait()


def local(
    queries,
    cell_key_rows,
    cell_value_rows,
    output_gate_logits,
    input_gate_logs,
    forget_gate_logits,
    extra_log_forget,
    head_norm_gain,
    cell_output_matrix,
    residual,
    expert_norm_gain,
    routes,
    token_expert_weights,
    expert_gate_matrix,
    expert_up_matrix,
    expert_down_matrix,
):
    vmem = pl.BlockSpec(memory_space=pltpu.VMEM)
    hbm = pl.BlockSpec(memory_space=pltpu.HBM)
    dma = pltpu.SemaphoreType.DMA
    width = GROUPS * WIDE
    return pl.pallas_call(
        kernel,
        name="layer",
        out_shape=jax.ShapeDtypeStruct((TOK, width), BF16),
        in_specs=[vmem] * 11 + [hbm] * 5,
        out_specs=vmem,
        scratch_shapes=[
            pltpu.VMEM((2, HEAD_DIM, width), BF16),
            pltpu.VMEM((4, width, HEAD_DIM), BF16),
            pltpu.VMEM((2, HEAD_DIM, width), BF16),
            pltpu.VMEM((TOK, width), BF16),
            pltpu.VMEM((NX, HEAD_DIM + 8, HEAD_DIM), F32),
            pltpu.VMEM((HEAD_DIM + 8, HEAD_DIM), F32),
            pltpu.VMEM((NX, HEAD_DIM + 8, HEAD_DIM), F32),
            pltpu.VMEM((NSP, 8, HEAD_DIM), F32),
            pltpu.VMEM((LEN, HEAD_DIM), F32),
            pltpu.VMEM((LEN, HEAD_DIM), F32),
            pltpu.VMEM((LEN // 2, HEAD_DIM), F32),
            pltpu.VMEM((LEN // 2, HEAD_DIM), F32),
            pltpu.VMEM((LEN // 2, HEAD_DIM), BF16),
            pltpu.VMEM((LEN // 2, HEAD_DIM), BF16),
            pltpu.VMEM((NZ, TROWS, WIDE), F32),
            pltpu.VMEM((2, 4, TROWS, WIDE), BF16),
            pltpu.VMEM((2, 4, TROWS, WIDE), BF16),
            pltpu.VMEM((TROWS, WIDE), BF16),
            pltpu.VMEM((TURNS + 1, ROWS, WIDE), BF16),
            pltpu.VMEM((TURNS + 1, ROWS, WIDE), BF16),
            pltpu.VMEM((HROWS, WIDE), BF16),
            pltpu.VMEM((ROWS, ROWS), BF16),
            pltpu.VMEM((ROWS, ROWS), BF16),
            pltpu.VMEM((ROWS, HROWS), BF16),
            pltpu.VMEM((ROWS, HROWS), BF16),
            pltpu.VMEM((LEN, HEAD_DIM), F32),
            pltpu.VMEM((NZ, TURNS, ROWS, WIDE), BF16),
            pltpu.VMEM((PER, 4 * HEAD_DIM), F32),
            pltpu.VMEM((PER, WIDE), F32),
            pltpu.VMEM((TURNS, ROWS, WIDE), BF16),
            pltpu.VMEM((2 * HROWS, ROWS), BF16),
            pltpu.VMEM((NZ, TURNS, ROWS, WIDE), BF16),
            pltpu.VMEM((NZ, TURNS, ROWS, WIDE), BF16),
            pltpu.VMEM((NZ, TURNS, HROWS, WIDE), BF16),
            pltpu.VMEM((NZ + 1, TURNS, HROWS, WIDE), BF16),
            pltpu.VMEM((TURNS, HROWS, WIDE), F32),
            dma((5,)), dma((4,)), dma((4,)), dma((NX,)), dma((NX,)), dma((NX,)), dma((NX,)), dma((2,)),
            dma((2, 4, STRIPES)), dma((2, 4, STRIPES)),
            dma((TURNS + 1,)), dma((TURNS + 1,)), dma((2,)),
            dma((NZ - 1, TURNS, PIECES)), dma((NZ - 1, TURNS, PIECES)),
            dma((NZ, TURNS)), dma((NZ, TURNS)), dma((NZ, TURNS)), dma((NZ + 1, TURNS)),
        ],
        compiler_params=pltpu.CompilerParams(
            collective_id=0, has_side_effects=True, vmem_limit_bytes=60 << 20
        ),
    )(
        queries,
        cell_key_rows,
        cell_value_rows,
        output_gate_logits,
        input_gate_logs,
        forget_gate_logits,
        extra_log_forget,
        head_norm_gain.reshape(1, HEAD_DIM),
        expert_norm_gain.reshape(1, width),
        routes.T,
        token_expert_weights.T,
        residual,
        cell_output_matrix,
        expert_gate_matrix[0],
        expert_up_matrix[0],
        expert_down_matrix[0],
    )


def solution(mesh):
    in_specs = (
        P("sp", "tp"),
        P("sp", "tp"),
        P("sp", "tp"),
        P("sp", "tp"),
        P("tp", "sp"),
        P("tp", "sp"),
        P("tp", "sp"),
        P("tp"),
        P("tp", None),
        P("sp", None),
        P(),
        P("sp", None),
        P("sp", None),
        P("sp", None, "tp"),
        P("sp", None, "tp"),
        P("sp", "tp", None),
    )
    return jax.shard_map(
        local, mesh=mesh, in_specs=in_specs, out_specs=P(("sp", "tp"), None), check_vma=False
    )
```
